256 devices in a mesh: ep: 64 (over z, x, core), tp: 4 (over y).
Axes of the slice: x: 4, y: 4, z: 8, core: 2. Of those that a mesh axis runs over, the one named last changes fastest.
Arguments:
- mixer_input: bfloat16 [32768, 2048], P('ep'), may hold values from -6 to 6
- mixer_gain: float32 [2048], replicated, may hold values from 0.1 to 1.9
- query_weight: bfloat16 [2048, 1024], P(None, 'tp'), may hold values from -0.125 to 0.125
- key_weight: bfloat16 [2048, 1024], P(None, 'tp'), may hold values from -0.125 to 0.125
- value_weight: bfloat16 [2048, 1024], P(None, 'tp'), may hold values from -0.125 to 0.125
- gate_weight: bfloat16 [2048, 1024], P(None, 'tp'), may hold values from -0.125 to 0.125
- head_gain: float32 [1024], P('tp'), may hold values from 0.1 to 1.9
- output_weight: bfloat16 [1024, 2048], P('tp'), may hold values from -0.1875 to 0.1875
- log_decay: float32 [32768, 8], P('ep', 'tp'), may hold values from -1 to 0, as said below
- expert_input: bfloat16 [32768, 2048], P(('ep', 'tp')), may hold values from -6 to 6
- expert_gain: float32 [2048], replicated, may hold values from 0.1 to 1.9
- routes: int32 [32768, 2], P(('ep', 'tp')), may hold values from 0 to 63, all different within a row; in each aligned block of 128 rows (0 to 127, 128 to 255, ...) at most 6 rows name the same one
- route_weight: float32 [32768, 2], P(('ep', 'tp')), may hold values from 0.1 to 1
- expert_gate: bfloat16 [64, 2048, 1024], P('ep', None, 'tp'), may hold values from -0.125 to 0.125
- expert_up: bfloat16 [64, 2048, 1024], P('ep', None, 'tp'), may hold values from -0.125 to 0.125
- expert_down: bfloat16 [64, 1024, 2048], P('ep', 'tp'), may hold values from -0.1875 to 0.1875
Outputs:
- mixer_output: bfloat16 [32768, 2048], P(('ep', 'tp'))
- expert_output: bfloat16 [32768, 2048], P(('ep', 'tp'))
The draws below stay inside these ranges and needn't reach their ends.
Inputs may be any that keep to these rules, and one draw needn't show every extreme that they name: `routes`: each row names 2 different experts. Among the rows of one device no expert is named more than 6 times, and in every draw the rows of some device name some expert exactly 6 times. `log_decay`: negative values.
All inputs are finite; a program needn't handle non-finite values.
Results may differ from the reference program's by a relative error of at most 0.025.
Values may be sent and summed in bfloat16 or wider, within the bound.
A program may use at most 128 MiB of HBM per device.

```python
import math
import jax
import jax.numpy as jnp
import numpy as np
from jax import lax

D = 2048
HEADS = 8
HEAD_DIM = 128
FF = 1024
BLOCK = 128
TOPK = 2
TOK_A = 512
TOK_B = 128
RET_WIDTH = 1024
TOKENS_A = 32768
TOKENS_B = 32768
EXPERTS = 64
CAP = 6
N_EP = 64
N_TP = 4


def draw_log_decay(key, part):
    symbol_strings = jax.random.split(key, 7)
    series_extent = TOKENS_A
    fast_share = 50
    fast_heads = jax.random.randint(symbol_strings[0], (HEADS,), 0, 100) < fast_share
    fast_rate = 1.0 / jax.random.uniform(symbol_strings[1], (HEADS,), jnp.float32, 30.0, 60.0)
    slow_rate = 2.302585 * jax.random.uniform(symbol_strings[2], (HEADS,), jnp.float32, 0.3, 1.0) / (2.5 * series_extent)
    rate = jnp.where(fast_heads, fast_rate, slow_rate)
    shard_factor = jnp.repeat(jax.random.uniform(symbol_strings[3], (N_EP,), jnp.float32, 1.0, 2.5), TOK_A)
    rough = jax.random.uniform(symbol_strings[4], (series_extent, HEADS), jnp.float32, 0.5, 1.5)
    default_fading_exponent = -rate[None, :] * shard_factor[:, None] * rough
    spike_offset = jax.random.randint(symbol_strings[5], (3,), 0, series_extent)
    objective_scores = jax.random.uniform(symbol_strings[6], (3, HEADS), jnp.float32, 0.2, 0.4)
    agreeing_tally = (jnp.arange(series_extent, dtype=jnp.int32)[:, None] == spike_offset[None, :]).astype(jnp.float32)
    spike_clusters = jnp.sum(agreeing_tally[:, :, None] * jnp.log(1.0 - objective_scores)[None, :, :], axis=1)
    return (default_fading_exponent + spike_clusters).astype(jnp.float32)


def block_scale(key, extent, pieces, least, top_value):
    def one(dim, parts):
        heights = jax.random.uniform(jax.random.fold_in(jax.random.fold_in(key, 6), dim), (parts,), jnp.float32, least / len(pieces), top_value / len(pieces))
        return jnp.repeat(jnp.exp(heights), extent[dim] // parts).reshape((-1,) + (1,) * (len(extent) - dim - 1))

    loudness = one(*pieces[0])
    for cut in pieces[1:]:
        loudness = loudness * one(*cut)
    return loudness


def routed_block(own_key, own, number, rows, count, top, bound, lean):
    ranking = jax.random.permutation(own_key, count)
    packed, common = shares(count, rows * top, bound, lean, True), shares(count, rows * top, bound, lean, False)
    places = jnp.arange(count)

    def named(tallies, rotation):
        used = int((tallies > 0).sum())
        fixed = max(1, used // 4)
        moved = fixed + (places - fixed + rotation * (used - fixed)) % max(1, count - fixed)
        return jnp.zeros((count,), jnp.int32).at[ranking[jnp.where(places < fixed, places, moved)]].set(jnp.asarray(tallies, jnp.int32))

    tallies = jnp.where(number % 4 == 0, named(packed, number // 4), named(common, number - number // 4 - 1))
    mixed = jax.random.permutation(jax.random.fold_in(own, 3), count)
    donor, taker = mixed[0:count // 2 * 2:2], mixed[1:count // 2 * 2:2]
    margin = jnp.minimum(tallies[donor] - 1, bound - tallies[taker]) // 2
    margin = jnp.where((donor == ranking[0]) | (taker == ranking[0]) | (tallies[taker] == 0), 0, jnp.maximum(margin, 0))
    moved = jax.random.randint(jax.random.fold_in(own, 4), (count // 2,), 0, 1 << 20) % (margin + 1)
    tallies = tallies.at[donor].add(-moved).at[taker].add(moved)
    labels = jnp.searchsorted(jnp.cumsum(tallies), jnp.arange(rows * top), side="right").astype(jnp.int32)
    listing = labels.reshape(top, rows).T
    listing = listing[jax.random.permutation(jax.random.fold_in(own, 1), rows)]
    rotation = jax.random.randint(jax.random.fold_in(own, 2), (rows, 1), 0, top)
    return jnp.take_along_axis(listing, (jnp.arange(top)[None, :] + rotation) % top, axis=1)


def shares(number_of, total, most, skew, full):
    portions = [(1 << 20) // math.isqrt(standing ** skew) + 1 for standing in range(1, number_of + 1)]
    largest = most if full else min(most, max(-(-total // number_of), total * portions[0] // sum(portions)))
    least = 1 if total - largest >= number_of - 1 else 0
    given, spare = [largest] + [least] * (number_of - 1), total - largest - least * (number_of - 1)
    while spare > 0:
        candidates = [i for i in range(1, number_of) if given[i] < largest] or [i for i in range(1, number_of) if given[i] < most]
        mass, budget = sum([portions[i] for i in candidates]), spare
        for i in candidates:
            more = min(most - given[i], max(1, budget * portions[i] // mass), spare)
            given[i] = given[i] + more
            spare = spare - more
    return np.array(given)


def gaussian(rng, dims, deviation, most, pieces=(), held_as=jnp.bfloat16):
    values = deviation * jax.random.normal(rng, dims, jnp.float32)
    if pieces:
        values = values * block_scale(rng, dims, pieces, -0.22, 0.18)
    return jnp.clip(values, -most, most).astype(held_as)


def setup_inputs(seed: int = 0) -> dict:
    splits = jax.random.split(jax.random.key(seed), 17)
    mixer_input = gaussian(splits[0], (TOKENS_A, D), 1.0, 6.0, ((0, 64),))
    mixer_gain = jnp.clip(1.0 + 0.18 * jax.random.normal(splits[1], (D,), jnp.float32), 0.1, 1.9)
    query_weight = gaussian(splits[2], (D, RET_WIDTH), D ** -0.5, 0.125, ((1, 4),))
    key_weight = gaussian(splits[3], (D, RET_WIDTH), D ** -0.5, 0.125, ((1, 4),))
    value_weight = gaussian(splits[4], (D, RET_WIDTH), D ** -0.5, 0.125, ((1, 4),))
    gate_weight = gaussian(splits[5], (D, RET_WIDTH), D ** -0.5, 0.125, ((1, 4),))
    head_gain = jnp.clip(1.0 + 0.18 * jax.random.normal(splits[6], (RET_WIDTH,), jnp.float32), 0.1, 1.9)
    output_weight = gaussian(splits[7], (RET_WIDTH, D), RET_WIDTH ** -0.5, 0.1875, ((0, 4),))
    log_decay = draw_log_decay(jax.random.fold_in(splits[16], 71), 0)
    expert_input = gaussian(splits[9], (TOKENS_B, D), 1.0, 6.0, ((0, 256),))
    expert_gain = jnp.clip(1.0 + 0.18 * jax.random.normal(splits[10], (D,), jnp.float32), 0.1, 1.9)
    routes_keys = jax.random.split(jax.random.fold_in(splits[11], 1), TOKENS_B // TOK_B)
    routes_turns = jax.random.permutation(jax.random.fold_in(splits[11], 3), TOKENS_B // TOK_B)
    routes = jax.vmap(lambda own, number: routed_block(jax.random.fold_in(splits[11], 2), own, number, TOK_B, EXPERTS, TOPK, CAP, 1))(routes_keys, routes_turns).reshape((TOKENS_B, TOPK))
    route_weight = jnp.clip(0.1 + 0.9 * jax.random.uniform(splits[12], (TOKENS_B, TOPK), jnp.float32) ** block_scale(splits[12], (TOKENS_B, TOPK), ((0, 256),), -0.2, 0.2), 0.1, 1.0)
    expert_gate = gaussian(splits[13], (EXPERTS, D, FF), D ** -0.5, 0.125, ((0, 64), (2, 4)))
    expert_up = gaussian(splits[14], (EXPERTS, D, FF), D ** -0.5, 0.125, ((0, 64), (2, 4)))
    expert_down = gaussian(splits[15], (EXPERTS, FF, D), FF ** -0.5, 0.1875, ((0, 64), (1, 4)))
    return dict(mixer_input=mixer_input, mixer_gain=mixer_gain, query_weight=query_weight, key_weight=key_weight, value_weight=value_weight, gate_weight=gate_weight, head_gain=head_gain, output_weight=output_weight, log_decay=log_decay, expert_input=expert_input, expert_gain=expert_gain, routes=routes, route_weight=route_weight, expert_gate=expert_gate, expert_up=expert_up, expert_down=expert_down)


EPS = 1e-06
HIGH = lax.Precision.HIGHEST

def norm_rows(values, gain):
    floats = values.astype(jnp.float32)
    scale = lax.rsqrt(lax.optimization_barrier(jnp.mean(floats * floats, axis=-1, keepdims=True)) + EPS)
    return (floats * scale * gain).astype(jnp.bfloat16)

def rotate(values, position):
    half_dim = values.shape[-1] // 2
    frequency = 10000.0 ** (-jnp.arange(half_dim, dtype=jnp.float32) / half_dim)
    angles = position.astype(jnp.float32)[:, None] * frequency[None, :]
    cosine = jnp.cos(angles)[:, None, :]
    sine_part = jnp.sin(angles)[:, None, :]
    first_half = values[..., :half_dim]
    second = values[..., half_dim:]
    return jnp.concatenate([first_half * cosine - second * sine_part, first_half * sine_part + second * cosine], axis=-1)

def lifted(array):
    return lax.optimization_barrier(array).astype(jnp.float32)

def retain(q_rot, k_rot, values_new, log_decay):
    series_extent, head_count, head_dim = q_rot.shape
    block_count = series_extent // BLOCK
    row_ids = lax.broadcasted_iota(jnp.int32, (BLOCK, BLOCK), 0)
    col_ids = lax.broadcasted_iota(jnp.int32, (BLOCK, BLOCK), 1)
    lower_mask = col_ids <= row_ids
    triangle = lower_mask.astype(jnp.float32)

    def shaped(array):
        return array.reshape((block_count, BLOCK) + array.shape[1:])

    def advance(carry_state, inputs):
        q_block, k_block, v_block, step_block = inputs
        cumulative = jnp.einsum('ij,jh->hi', triangle, step_block, precision=HIGH)
        block_total = cumulative[:, -1]
        differences = cumulative[:, :, None] - cumulative[:, None, :]
        decays = jnp.where(lower_mask, jnp.exp(jnp.where(lower_mask, differences, 0.0)), 0.0)
        q_float = q_block.astype(jnp.float32)
        k_float = k_block.astype(jnp.float32)
        v_float = v_block.astype(jnp.float32)
        scores = jnp.einsum('ihd,jhd->hij', q_float, k_float, precision=HIGH)
        weights = lifted((scores * decays).astype(jnp.bfloat16))
        inner_term = jnp.einsum('hij,jhe->ihe', weights, v_float, precision=HIGH)
        cross_term = jnp.einsum('hi,ihd,hde->ihe', jnp.exp(cumulative), q_float, carry_state, precision=HIGH)
        key_scale = jnp.exp(block_total[:, None] - cumulative)
        updates = jnp.einsum('hj,jhd,jhe->hde', key_scale, k_float, v_float, precision=HIGH)
        next_state = jnp.exp(block_total)[:, None, None] * carry_state + updates
        return (next_state, inner_term + cross_term)
    initial = jnp.zeros((head_count, head_dim, head_dim), jnp.float32)
    _, outputs = lax.scan(advance, initial, (shaped(q_rot), shaped(k_rot), shaped(values_new), shaped(log_decay)))
    return outputs.reshape(series_extent, head_count, head_dim)

def reference(mixer_input, mixer_gain, query_weight, key_weight, value_weight, gate_weight, head_gain, output_weight, log_decay, expert_input, expert_gain, routes, route_weight, expert_gate, expert_up, expert_down):
    series_extent = mixer_input.shape[0]
    normed = norm_rows(mixer_input, mixer_gain)

    def project(weight):
        return jnp.dot(normed, weight, preferred_element_type=jnp.float32).astype(jnp.bfloat16)
    queries = project(query_weight)
    keys_raw = project(key_weight)
    values_new = project(value_weight)
    gate_raw = project(gate_weight)
    position = jnp.arange(series_extent, dtype=jnp.int32)
    q_rot = rotate(lifted(queries).reshape(series_extent, HEADS, HEAD_DIM), position).astype(jnp.bfloat16)
    k_rot = (rotate(lifted(keys_raw).reshape(series_extent, HEADS, HEAD_DIM), position) * HEAD_DIM ** (-0.5)).astype(jnp.bfloat16)
    retained = retain(q_rot, k_rot, values_new.reshape(series_extent, HEADS, HEAD_DIM), log_decay)
    centre = lax.optimization_barrier(jnp.mean(retained, axis=-1, keepdims=True))
    spread = lax.optimization_barrier(jnp.mean(jnp.square(retained - centre), axis=-1, keepdims=True))
    scaled = (retained - centre) * lax.rsqrt(spread + EPS) * head_gain.reshape(HEADS, HEAD_DIM)
    gated = scaled.reshape(series_extent, RET_WIDTH) * jax.nn.silu(lifted(gate_raw))
    mixer_hidden = gated.astype(jnp.bfloat16)
    quarter = RET_WIDTH // N_TP
    running = jnp.zeros((series_extent, D), jnp.float32)
    for group_index in range(N_TP):
        group_term = jnp.dot(mixer_hidden[:, group_index * quarter:(group_index + 1) * quarter], output_weight[group_index * quarter:(group_index + 1) * quarter], preferred_element_type=jnp.float32)
        running = running + lifted(group_term.astype(jnp.bfloat16))
    mixer_output = running.astype(jnp.bfloat16)
    expert_normed = norm_rows(expert_input, expert_gain)
    block_count = N_EP * N_TP
    entry_count = TOK_B * TOPK
    flat_routes = routes.reshape(block_count, entry_count)
    onehot = (flat_routes[:, :, None] == jnp.arange(EXPERTS, dtype=jnp.int32)[None, None, :]).astype(jnp.int32)
    prior_count = jnp.cumsum(onehot, axis=1) - onehot
    slot_index = lax.optimization_barrier(jnp.sum(prior_count * onehot, axis=2)).astype(jnp.int32)
    block_ids = jnp.broadcast_to(jnp.arange(block_count, dtype=jnp.int32)[:, None], (block_count, entry_count))
    entry_ids = block_ids * entry_count + jnp.arange(entry_count, dtype=jnp.int32)[None, :]
    slot_table = jnp.full((EXPERTS, block_count, CAP), -1, jnp.int32).at[flat_routes, block_ids, slot_index].set(entry_ids)
    norm_weight = route_weight / lax.optimization_barrier(jnp.sum(route_weight, axis=1, keepdims=True))
    flat_weight = norm_weight.reshape(-1)

    def per_expert(running_sum, inputs):
        gate_w, up_w, down_w, id_table = inputs
        id_list = id_table.reshape(-1)
        valid = id_list >= 0
        safe_ids = jnp.where(valid, id_list, 0).astype(jnp.int32)
        tok_index = (safe_ids // TOPK).astype(jnp.int32)
        rows_in = jnp.where(valid[:, None], expert_normed[tok_index], jnp.zeros((), jnp.bfloat16))
        gate_part = jnp.dot(rows_in, gate_w, preferred_element_type=jnp.float32)
        up_part = jnp.dot(rows_in, up_w, preferred_element_type=jnp.float32)
        hidden = (jax.nn.silu(gate_part) * up_part).astype(jnp.bfloat16)
        result = lifted(jnp.dot(hidden, down_w, preferred_element_type=jnp.float32).astype(jnp.bfloat16))
        scale = jnp.where(valid, flat_weight[safe_ids], 0.0)
        return (running_sum.at[tok_index].add(scale[:, None] * result), None)
    total, _ = lax.scan(per_expert, jnp.zeros((TOKENS_B, D), jnp.float32), (expert_gate, expert_up, expert_down, slot_table))
    expert_output = total.astype(jnp.bfloat16)
    return (mixer_output, expert_output)
```

```python
import functools

import jax
import jax.numpy as jnp
from jax import lax
from jax.experimental import pallas as pl
from jax.experimental.pallas import tpu as pltpu
from jax.sharding import Mesh
from jax.sharding import PartitionSpec as P

BLOCK = 128
EP = ("ep_0", "ep_1", "ep_2")
EP_TP = ("ep_0", "ep_1", "ep_2", "tp")


EPS = 1e-06


def filled_with(x, identity):
    return jax.tree.map(
        lambda part, zero: jnp.zeros_like(part) + jnp.asarray(zero, part.dtype), x, identity
    )


def carried_in(x, axes, combine, identity):
    before = start = filled_with(x, identity)
    running = x
    for axis in reversed(axes):
        peers, position = (lax.axis_size(axis), lax.axis_index(axis))
        pieces = jax.tree.map(
            lambda part, kind: lax.all_gather(part.astype(kind), axis),
            running,
            (jnp.bfloat16, jnp.bfloat16),
        )
        inside, running = (start, start)
        for k in range(peers):
            passed = k < position
            running = combine(
                running, jax.tree.map(lambda part, own: part[k].astype(own.dtype), pieces, x)
            )
            inside = jax.tree.map(lambda new, old: jnp.where(passed, new, old), running, inside)
        before = combine(inside, before)
    return before


def norm_rows(values, gain):
    floats = values.astype(jnp.float32)
    scale = lax.rsqrt(jnp.mean(floats * floats, axis=-1, keepdims=True) + EPS)
    return (floats * scale * gain).astype(jnp.bfloat16)


def rotate(values, position):
    half_dim = values.shape[-1] // 2
    frequency = 10000.0 ** (-jnp.arange(half_dim, dtype=jnp.float32) / half_dim)
    angles = position.astype(jnp.float32)[:, None] * frequency[None, :]
    cosine = jnp.cos(angles)[:, None, :]
    sine_part = jnp.sin(angles)[:, None, :]
    first_half = values[..., :half_dim]
    second = values[..., half_dim:]
    return jnp.concatenate(
        [first_half * cosine - second * sine_part, first_half * sine_part + second * cosine],
        axis=-1,
    )


def chain_pair(earlier, following):
    return (earlier[0] * following[0], following[0][:, None, None] * earlier[1] + following[1])


def mixer_half(
    mixer_input,
    mixer_gain,
    query_weight,
    key_weight,
    value_weight,
    gate_weight,
    head_gain,
    output_weight,
    log_decay,
):
    row_count = mixer_input.shape[0]
    head_count = log_decay.shape[1]
    mix_width = query_weight.shape[1]
    head_dim = mix_width // head_count
    normed = norm_rows(mixer_input, mixer_gain)

    def project(weight):
        return jnp.dot(normed, weight, preferred_element_type=jnp.float32).astype(jnp.bfloat16)

    queries = project(query_weight)
    keys_raw = project(key_weight)
    values_new = project(value_weight)
    gate_raw = project(gate_weight)
    position = lax.axis_index(EP) * row_count + jnp.arange(row_count, dtype=jnp.int32)
    q_rot = rotate(
        queries.astype(jnp.float32).reshape(row_count, head_count, head_dim), position
    ).astype(jnp.bfloat16)
    k_rot = (
        rotate(keys_raw.astype(jnp.float32).reshape(row_count, head_count, head_dim), position)
        * head_dim ** (-0.5)
    ).astype(jnp.bfloat16)
    block_count = row_count // BLOCK
    q_blocks = q_rot.reshape(block_count, BLOCK, head_count, head_dim)
    k_blocks = k_rot.reshape(block_count, BLOCK, head_count, head_dim)
    v_blocks = values_new.reshape(block_count, BLOCK, head_count, head_dim)
    log_steps = log_decay.reshape(block_count, BLOCK, head_count)
    row_ids = lax.broadcasted_iota(jnp.int32, (BLOCK, BLOCK), 0)
    col_ids = lax.broadcasted_iota(jnp.int32, (BLOCK, BLOCK), 1)
    lower_mask = col_ids <= row_ids
    cumulative = jnp.einsum("ij,bjh->bhi", lower_mask.astype(jnp.float32), log_steps)
    block_total = cumulative[:, :, -1]
    differences = cumulative[:, :, :, None] - cumulative[:, :, None, :]
    decays = jnp.where(lower_mask, jnp.exp(jnp.where(lower_mask, differences, 0.0)), 0.0)
    scores = jnp.einsum("bihd,bjhd->bhij", q_blocks, k_blocks, preferred_element_type=jnp.float32)
    weights = (scores * decays).astype(jnp.bfloat16)
    inner_term = jnp.einsum(
        "bhij,bjhe->bihe", weights, v_blocks, preferred_element_type=jnp.float32
    )
    key_scale = jnp.exp(block_total[:, :, None] - cumulative)
    updates = jnp.einsum(
        "bhj,bjhd,bjhe->bhde", key_scale, k_blocks.astype(jnp.float32), v_blocks.astype(jnp.float32)
    )
    factor = jnp.exp(block_total)
    local_state = jnp.zeros((head_count, head_dim, head_dim), jnp.float32)
    for block_index in range(block_count):
        local_state = factor[block_index][:, None, None] * local_state + updates[block_index]
    entering = carried_in(
        (jnp.exp(jnp.sum(block_total, axis=0)), local_state),
        EP,
        chain_pair,
        (jnp.ones((head_count,), jnp.float32), jnp.zeros_like(local_state)),
    )
    carry_state = entering[1]
    starts = []
    for block_index in range(block_count):
        starts.append(carry_state)
        carry_state = factor[block_index][:, None, None] * carry_state + updates[block_index]
    carried = jnp.stack(starts)
    cross_term = jnp.einsum(
        "bhi,bihd,bhde->bihe", jnp.exp(cumulative), q_blocks.astype(jnp.float32), carried
    )
    retained = (inner_term + cross_term).reshape(row_count, head_count, head_dim)
    centre = jnp.mean(retained, axis=-1, keepdims=True)
    spread = jnp.mean(jnp.square(retained - centre), axis=-1, keepdims=True)
    scaled = (retained - centre) * lax.rsqrt(spread + EPS) * head_gain.reshape(head_count, head_dim)
    mixer_hidden = (
        scaled.reshape(row_count, mix_width) * jax.nn.silu(gate_raw.astype(jnp.float32))
    ).astype(jnp.bfloat16)
    return lax.psum_scatter(
        jnp.dot(mixer_hidden, output_weight, preferred_element_type=jnp.float32).astype(
            jnp.bfloat16
        ),
        "tp",
        scatter_dimension=0,
        tiled=True,
    )


CAP = 6
MESH_ID = pl.DeviceIdType.MESH
VMEM_LIMIT = 64 * 1024 * 1024 - 1024 * 1024


def z_order(count):
    steps = []
    for k in range(1, count // 2 + 1):
        steps.append(k)
        if count - k != k:
            steps.append(count - k)
    return steps + [0]


def place():
    sizes = tuple(lax.axis_size(name) for name in EP)
    spots = tuple(lax.axis_index(name) for name in EP)
    return sizes, spots


def for_each_peer(body):
    (nz, nx, nc), (z, x, c) = place()

    def step(i, carry):
        tx = lax.rem(x + i // nc, nx)
        tc = lax.rem(c + i % nc, nc)
        for offset in z_order(nz):
            tz = lax.rem(z + offset, nz)
            call = functools.partial(
                body, {"ep_0": tz, "ep_1": tx, "ep_2": tc}, (tz * nx + tx) * nc + tc
            )
            if offset == 0:
                pl.when(i > 0)(call)
            else:
                call()
        return carry

    lax.fori_loop(0, nx * nc, step, 0)


def remote(src, dst, send_sem, recv_sem, device):
    return pltpu.make_async_remote_copy(
        src_ref=src,
        dst_ref=dst,
        send_sem=send_sem,
        recv_sem=recv_sem,
        device_id=device,
        device_id_type=MESH_ID,
    )


def wait_bytes(ref, sem):
    pltpu.make_async_copy(ref, ref, sem).wait()


def packed_ids(shape, dim, piece):
    row = lax.broadcasted_iota(jnp.int32, shape, dim)
    owner = (row // 8) * CAP
    lane = row % 8
    if piece is None:
        return jnp.where(lane < CAP, owner + lane, -1)
    return jnp.where(lane == 6, owner + piece, jnp.where(lane == 7, owner + 3 + piece, -1))


def dot(a, b):
    return jnp.dot(a, b, preferred_element_type=jnp.float32)


def expert_kernel(
    x_ref,
    gain_ref,
    routes_ref,
    score_ref,
    gate_hbm,
    up_hbm,
    down_hbm,
    out_ref,
    send_buf,
    arrived,
    rows,
    gate_buf,
    up_buf,
    down_buf,
    hidden,
    part_send,
    part_recv,
    back_send,
    back,
    weigh,
    dispatch_send,
    dispatch_recv,
    forward_send,
    forward_recv,
    weight_send,
    weight_recv,
    weight_local,
    part_send_sem,
    part_recv_sem,
    back_send_sem,
    back_recv_sem,
    own_sem,
):
    (nz, nx, nc), (z, x, c) = place()
    me = (z * nx + x) * nc + c
    y = lax.axis_index("tp")
    flip, mirror = y + 1 - 2 * (y % 2), 3 - y
    weight_peer = {"tp": (1 - c) * flip + c * mirror}
    token_peer = {"tp": (1 - c) * mirror + c * flip}
    experts = nz * nx * nc
    tokens, width = x_ref.shape
    piece = width // 4
    row_count = experts * CAP
    group = min(32, experts)
    group_count = experts // group

    barrier = pltpu.get_barrier_semaphore()
    for_each_peer(
        lambda device, index: pl.semaphore_signal(
            barrier, inc=1, device_id=device, device_id_type=MESH_ID
        )
    )
    for peer in (weight_peer, token_peer):
        pl.semaphore_signal(barrier, inc=1, device_id=peer, device_id_type=MESH_ID)
    locals_ = []
    for k, (source, target) in enumerate(
        ((gate_hbm, gate_buf), (up_hbm, up_buf), (down_hbm, down_buf))
    ):
        locals_.append(pltpu.make_async_copy(source, target.at[0], weight_local.at[k]))
        locals_[-1].start()
    pl.semaphore_wait(barrier, experts + 1)

    weights_out = [
        remote(gate_hbm, gate_buf.at[1], weight_send.at[0], weight_recv.at[0], weight_peer),
        remote(up_hbm, up_buf.at[1], weight_send.at[1], weight_recv.at[1], weight_peer),
        remote(down_hbm, down_buf.at[1], weight_send.at[2], weight_recv.at[2], weight_peer),
    ]
    for copy in weights_out:
        copy.start()

    floats = x_ref[...].astype(jnp.float32)
    scale = lax.rsqrt(jnp.mean(floats * floats, axis=-1, keepdims=True) + EPS)
    normed = (floats * scale * gain_ref[...]).astype(jnp.bfloat16)

    entries = 2 * tokens
    routes = routes_ref[...]
    named = lax.broadcasted_iota(jnp.int32, (experts, entries), 0) == routes
    named_bf = jnp.where(named, 1.0, 0.0).astype(jnp.bfloat16)
    earlier = lax.broadcasted_iota(jnp.int32, (entries, entries), 0) < lax.broadcasted_iota(
        jnp.int32, (entries, entries), 1
    )
    prior = dot(named_bf, jnp.where(earlier, 1.0, 0.0).astype(jnp.bfloat16))
    slot = jnp.sum(jnp.where(named, prior, 0.0), axis=0, keepdims=True).astype(jnp.int32)
    target = routes * CAP + slot
    first, second = target[:, :tokens], target[:, tokens:]
    scores = score_ref[...]
    shares = scores / jnp.sum(scores, axis=0, keepdims=True)

    packed = (8 * experts, tokens)
    ids = [packed_ids(packed, 0, j) for j in (None, 0, 1, 2)]
    picks = [
        jnp.where((i == first) | (i == second), 1.0, 0.0).astype(jnp.bfloat16) for i in ids
    ]
    last = normed[:, 3 * piece :]
    for j in range(3):
        chosen = jnp.concatenate([picks[0], picks[1 + j]], axis=1)
        source = jnp.concatenate([normed[:, j * piece : (j + 1) * piece], last], axis=0)
        send_buf[j] = dot(chosen, source).astype(jnp.bfloat16).reshape(experts, 8, piece)
        for_each_peer(
            lambda device, index, j=j: remote(
                send_buf.at[j, index],
                arrived.at[0, j, me],
                dispatch_send.at[j],
                dispatch_recv.at[j],
                device,
            ).start()
        )
        pltpu.make_async_copy(send_buf.at[j, me], arrived.at[0, j, me], own_sem.at[j]).start()

    for n, i in enumerate(ids):
        shared = jnp.where(i == first, shares[0:1], 0.0) + jnp.where(
            i == second, shares[1:2], 0.0
        )
        turned = shared.T
        high = turned.astype(jnp.bfloat16)
        weigh[n, 0] = high
        weigh[n, 1] = (turned - high.astype(jnp.float32)).astype(jnp.bfloat16)

    shape = (group * CAP, group * 8)
    spread = [
        jnp.where(
            packed_ids(shape, 1, j) == lax.broadcasted_iota(jnp.int32, shape, 0), 1.0, 0.0
        ).astype(jnp.bfloat16)
        for j in (None, 0, 1, 2)
    ]
    spread_last = jnp.concatenate(spread[1:], axis=1)

    def unpack(side, j):
        block = arrived[side, j].reshape(8 * experts, piece)
        for g in range(group_count):
            rows[side, g * group * CAP : (g + 1) * group * CAP, j * piece : (j + 1) * piece] = dot(
                spread[0], block[g * group * 8 : (g + 1) * group * 8]
            ).astype(jnp.bfloat16)

    def unpack_last(side):
        blocks = [arrived[side, j].reshape(8 * experts, piece) for j in range(3)]
        for g in range(group_count):
            stacked = jnp.concatenate(
                [block[g * group * 8 : (g + 1) * group * 8] for block in blocks], axis=0
            )
            rows[side, g * group * CAP : (g + 1) * group * CAP, 3 * piece :] = dot(
                spread_last, stacked
            ).astype(jnp.bfloat16)

    forwards = []
    for j in range(3):
        wait_bytes(send_buf.at[j, pl.ds(0, experts - 1)], dispatch_recv.at[j])
        pltpu.make_async_copy(send_buf.at[j, me], arrived.at[0, j, me], own_sem.at[j]).wait()
        forwards.append(
            remote(
                arrived.at[0, j],
                arrived.at[1, j],
                forward_send.at[j],
                forward_recv.at[j],
                token_peer,
            )
        )
        forwards[-1].start()
        unpack(0, j)
    unpack_last(0)

    def expand(side, half):
        source = rows[side]
        gate_part = dot(source, gate_buf[half])
        up_part = dot(source, up_buf[half])
        hidden[side, half] = (gate_part / (1.0 + jnp.exp(-gate_part)) * up_part).astype(
            jnp.bfloat16
        )

    locals_[0].wait()
    locals_[1].wait()
    expand(0, 0)
    for j in range(3):
        forwards[j].wait_recv()
        unpack(1, j)
    unpack_last(1)
    expand(1, 0)
    weights_out[0].wait_recv()
    weights_out[1].wait_recv()
    expand(1, 1)

    def contract(side, k):
        columns = slice(k * piece, (k + 1) * piece)
        return dot(hidden[side, 0], down_buf[0, :, columns]) + dot(
            hidden[side, 1], down_buf[1, :, columns]
        )

    locals_[2].wait()
    weights_out[2].wait_recv()
    parts = {}
    for k in (3, 0, 1, 2):
        part_send[k] = contract(1, k).astype(jnp.bfloat16)
        parts[k] = remote(
            part_send.at[k], part_recv.at[k], part_send_sem.at[k], part_recv_sem.at[k], token_peer
        )
        parts[k].start()
    expand(0, 1)

    def total(k):
        own = contract(0, k)
        parts[k].wait_recv()
        return (own + part_recv[k].astype(jnp.float32)).astype(jnp.bfloat16)

    gather = [
        jnp.where(
            packed_ids((group * 8, group * CAP), 0, j)
            == lax.broadcasted_iota(jnp.int32, (group * 8, group * CAP), 1),
            1.0,
            0.0,
        ).astype(jnp.bfloat16)
        for j in (None, 0, 1, 2)
    ]
    tail = total(3)
    for j in range(3):
        body = total(j)
        for g in range(group_count):
            span = slice(g * group * CAP, (g + 1) * group * CAP)
            back_send[j, g * group : (g + 1) * group] = (
                (dot(gather[0], body[span]) + dot(gather[1 + j], tail[span]))
                .astype(jnp.bfloat16)
                .reshape(group, 8, piece)
            )
        for_each_peer(
            lambda device, index, j=j: remote(
                back_send.at[j, index],
                back.at[j, me],
                back_send_sem.at[j],
                back_recv_sem.at[j],
                device,
            ).start()
        )
        pltpu.make_async_copy(back_send.at[j, me], back.at[j, me], own_sem.at[j]).start()

    rest = jnp.zeros((tokens, piece), jnp.float32)
    for j in range(3):
        wait_bytes(back_send.at[j, pl.ds(0, experts - 1)], back_recv_sem.at[j])
        pltpu.make_async_copy(back_send.at[j, me], back.at[j, me], own_sem.at[j]).wait()
        block = back[j].reshape(8 * experts, piece)
        out_ref[:, j * piece : (j + 1) * piece] = (
            dot(weigh[0, 0], block) + dot(weigh[0, 1], block)
        ).astype(jnp.bfloat16)
        rest = rest + dot(weigh[1 + j, 0], block) + dot(weigh[1 + j, 1], block)
    out_ref[:, 3 * piece :] = rest.astype(jnp.bfloat16)

    for copy in weights_out + forwards + list(parts.values()):
        copy.wait_send()
    for j in range(3):
        wait_bytes(send_buf.at[j, pl.ds(0, experts - 1)], dispatch_send.at[j])
        wait_bytes(back_send.at[j, pl.ds(0, experts - 1)], back_send_sem.at[j])


def expert_half(
    expert_input, expert_gain, routes, route_weight, expert_gate, expert_up, expert_down
):
    tokens, width = expert_input.shape
    experts = lax.axis_size(EP)
    shard = expert_gate.shape[2]
    piece = width // 4
    row_count = experts * CAP
    bf16 = jnp.bfloat16
    vmem = pl.BlockSpec(memory_space=pltpu.VMEM)
    anywhere = pl.BlockSpec(memory_space=pl.ANY)
    dma = pltpu.SemaphoreType.DMA
    return pl.pallas_call(
        expert_kernel,
        out_shape=jax.ShapeDtypeStruct((tokens, width), bf16),
        in_specs=[vmem] * 4 + [anywhere] * 3,
        out_specs=vmem,
        scratch_shapes=[
            pltpu.VMEM((3, experts, 8, piece), bf16),
            pltpu.VMEM((2, 3, experts, 8, piece), bf16),
            pltpu.VMEM((2, row_count, width), bf16),
            pltpu.VMEM((2, width, shard), bf16),
            pltpu.VMEM((2, width, shard), bf16),
            pltpu.VMEM((2, shard, width), bf16),
            pltpu.VMEM((2, 2, row_count, shard), bf16),
            pltpu.VMEM((4, row_count, piece), bf16),
            pltpu.VMEM((4, row_count, piece), bf16),
            pltpu.VMEM((3, experts, 8, piece), bf16),
            pltpu.VMEM((3, experts, 8, piece), bf16),
            pltpu.VMEM((4, 2, tokens, 8 * experts), bf16),
            dma((3,)),
            dma((3,)),
            dma((3,)),
            dma((3,)),
            dma((3,)),
            dma((3,)),
            dma((3,)),
            dma((4,)),
            dma((4,)),
            dma((3,)),
            dma((3,)),
            dma((3,)),
        ],
        compiler_params=pltpu.CompilerParams(
            collective_id=0, has_side_effects=True, vmem_limit_bytes=VMEM_LIMIT
        ),
        name="experts",
    )(
        expert_input,
        expert_gain.reshape(1, width),
        routes.T.reshape(1, -1),
        route_weight.T,
        expert_gate[0],
        expert_up[0],
        expert_down[0],
    )


def on_device(
    mixer_input,
    mixer_gain,
    query_weight,
    key_weight,
    value_weight,
    gate_weight,
    head_gain,
    output_weight,
    log_decay,
    expert_input,
    expert_gain,
    routes,
    route_weight,
    expert_gate,
    expert_up,
    expert_down,
):
    mixer_output = mixer_half(
        mixer_input,
        mixer_gain,
        query_weight,
        key_weight,
        value_weight,
        gate_weight,
        head_gain,
        output_weight,
        log_decay,
    )
    expert_output = expert_half(
        expert_input, expert_gain, routes, route_weight, expert_gate, expert_up, expert_down
    )
    return (mixer_output, expert_output)


def solution(mesh):
    finer = Mesh(mesh.devices.reshape(8, 4, 2, mesh.shape["tp"]), ("ep_0", "ep_1", "ep_2", "tp"))
    placed = (
        P(EP, None),
        P(),
        P(None, "tp"),
        P(None, "tp"),
        P(None, "tp"),
        P(None, "tp"),
        P("tp"),
        P("tp", None),
        P(EP, "tp"),
        P(EP_TP, None),
        P(),
        P(EP_TP, None),
        P(EP_TP, None),
        P(EP, None, "tp"),
        P(EP, None, "tp"),
        P(EP, "tp", None),
    )
    return jax.shard_map(
        on_device,
        mesh=finer,
        in_specs=placed,
        out_specs=(P(EP_TP, None), P(EP_TP, None)),
        check_vma=False,
    )
```

```python
import functools

import jax
import jax.numpy as jnp
from jax import lax
from jax.experimental import pallas as pl
from jax.experimental.pallas import tpu as pltpu
from jax.sharding import Mesh
from jax.sharding import PartitionSpec as P

BLOCK = 128
EP = ("ep_0", "ep_1", "ep_2")
EP_TP = ("ep_0", "ep_1", "ep_2", "tp")
EPS = 1e-06
CAP = 6
HEAD = 128
MESH_ID = pl.DeviceIdType.MESH
VMEM_LIMIT = 64 * 1024 * 1024 - 1024 * 1024


def z_order(count):
    steps = []
    for k in range(1, count // 2 + 1):
        steps.append(k)
        if count - k != k:
            steps.append(count - k)
    return steps + [0]


def place():
    sizes = tuple(lax.axis_size(name) for name in EP)
    spots = tuple(lax.axis_index(name) for name in EP)
    return sizes, spots


def for_each_peer(body):
    (nz, nx, nc), (z, x, c) = place()

    def step(i, carry):
        tx = lax.rem(x + i // nc, nx)
        tc = lax.rem(c + i % nc, nc)
        for offset in z_order(nz):
            tz = lax.rem(z + offset, nz)
            call = functools.partial(
                body, {"ep_0": tz, "ep_1": tx, "ep_2": tc}, (tz * nx + tx) * nc + tc
            )
            if offset == 0:
                pl.when(i > 0)(call)
            else:
                call()
        return carry

    lax.fori_loop(0, nx * nc, step, 0)


def remote(src, dst, send_sem, recv_sem, device):
    return pltpu.make_async_remote_copy(
        src_ref=src,
        dst_ref=dst,
        send_sem=send_sem,
        recv_sem=recv_sem,
        device_id=device,
        device_id_type=MESH_ID,
    )


def wait_bytes(ref, sem):
    pltpu.make_async_copy(ref, ref, sem).wait()


def packed_ids(shape, dim, piece):
    row = lax.broadcasted_iota(jnp.int32, shape, dim)
    owner = (row // 8) * CAP
    lane = row % 8
    if piece is None:
        return jnp.where(lane < CAP, owner + lane, -1)
    return jnp.where(lane == 6, owner + piece, jnp.where(lane == 7, owner + 3 + piece, -1))


def dot(a, b):
    return jnp.dot(a, b, preferred_element_type=jnp.float32)


def dot_t(a, b, dims):
    return lax.dot_general(a, b, (dims, ((), ())), preferred_element_type=jnp.float32)


def project_rows(mx_buf, mx_gain, mixer_weights, cos_ref, sin_ref, q_buf, k_buf, v_buf, g_buf):
    row_count, width = mx_buf.shape
    step_rows = min(256, row_count)
    heads = q_buf.shape[1] // HEAD

    def step(i, carry):
        span = pl.ds(pl.multiple_of(i * step_rows, step_rows), step_rows)
        floats = mx_buf[span, :].astype(jnp.float32)
        scale = lax.rsqrt(jnp.mean(floats * floats, axis=-1, keepdims=True) + EPS)
        normed = (floats * scale * mx_gain[...]).astype(jnp.bfloat16)
        cosine, sine = cos_ref[span, :], sin_ref[span, :]
        for n, target in enumerate((q_buf, k_buf, v_buf, g_buf)):
            raw = dot(normed, mixer_weights[n]).astype(jnp.bfloat16)
            if n >= 2:
                target[span, :] = raw
                continue
            for h in range(heads):
                part = raw[:, h * HEAD : (h + 1) * HEAD].astype(jnp.float32)
                swapped = jnp.concatenate([part[:, HEAD // 2 :], part[:, : HEAD // 2]], axis=1)
                turned = part * cosine + swapped * sine
                if n == 1:
                    turned = turned * HEAD ** (-0.5)
                target[span, h * HEAD : (h + 1) * HEAD] = turned.astype(jnp.bfloat16)
        return carry

    lax.fori_loop(0, row_count // step_rows, step, 0)


def scan_blocks(logs_ref, log_rows_ref, q_buf, k_buf, v_buf, inner_buf, update_buf, decay_buf):
    block_count = q_buf.shape[0] // BLOCK
    heads = q_buf.shape[1] // HEAD
    row_ids = lax.broadcasted_iota(jnp.int32, (BLOCK, BLOCK), 0)
    col_ids = lax.broadcasted_iota(jnp.int32, (BLOCK, BLOCK), 1)
    lower, upper = col_ids <= row_ids, row_ids <= col_ids

    def step(b, carry):
        span = pl.ds(pl.multiple_of(b * BLOCK, BLOCK), BLOCK)
        tall, wide = logs_ref[span, :], log_rows_ref[b]
        for h in range(heads):
            lanes = slice(h * HEAD, (h + 1) * HEAD)
            cum_col = jnp.sum(jnp.where(lower, wide[h : h + 1, :], 0.0), axis=1, keepdims=True)
            cum_row = jnp.sum(jnp.where(upper, tall[:, h : h + 1], 0.0), axis=0, keepdims=True)
            total = jnp.sum(wide[h : h + 1, :], axis=1, keepdims=True)
            q, k, v = q_buf[span, lanes], k_buf[span, lanes], v_buf[span, lanes]
            scaled = (k.astype(jnp.float32) * jnp.exp(total - cum_col)).astype(jnp.bfloat16)
            update_buf[b, h] = dot_t(scaled, v, ((0,), (0,)))
            decay_buf[b, h] = jnp.broadcast_to(total, (8, HEAD))
            decays = jnp.where(lower, jnp.exp(jnp.where(lower, cum_col - cum_row, 0.0)), 0.0)
            scores = dot_t(q, k, ((1,), (1,)))
            inner_buf[span, lanes] = dot((scores * decays).astype(jnp.bfloat16), v)
            q_buf[span, lanes] = (q.astype(jnp.float32) * jnp.exp(cum_col)).astype(jnp.bfloat16)
        return carry

    lax.fori_loop(0, block_count, step, 0)


def finish_blocks(
    entering, q_buf, g_buf, inner_buf, update_buf, decay_buf, head_gain, out_weight, out_buf
):
    block_count = q_buf.shape[0] // BLOCK
    heads = q_buf.shape[1] // HEAD

    def step(b, states):
        span = pl.ds(pl.multiple_of(b * BLOCK, BLOCK), BLOCK)
        following, hidden = [], []
        for h in range(heads):
            lanes = slice(h * HEAD, (h + 1) * HEAD)
            state = states[h]
            retained = inner_buf[span, lanes] + dot(q_buf[span, lanes], state.astype(jnp.bfloat16))
            factor = jnp.exp(decay_buf[b, h][0:1])
            following.append(factor * state + update_buf[b, h])
            centred = retained - jnp.mean(retained, axis=-1, keepdims=True)
            spread = jnp.mean(centred * centred, axis=-1, keepdims=True)
            gate = g_buf[span, lanes].astype(jnp.float32)
            hidden.append(
                (
                    centred
                    * lax.rsqrt(spread + EPS)
                    * head_gain[:, lanes]
                    * (gate / (1.0 + jnp.exp(-gate)))
                ).astype(jnp.bfloat16)
            )
        out_buf[span, :] = dot(jnp.concatenate(hidden, axis=1), out_weight[...]).astype(jnp.bfloat16)
        return tuple(following)

    lax.fori_loop(0, block_count, step, tuple(entering))


def layer_kernel(
    x_ref,
    gain_ref,
    routes_ref,
    score_ref,
    gate_hbm,
    up_hbm,
    down_hbm,
    mx_hbm,
    mx_gain,
    q_hbm,
    k_hbm,
    v_hbm,
    g_hbm,
    head_gain,
    o_hbm,
    logs_ref,
    log_rows_ref,
    cos_ref,
    sin_ref,
    mixed_ref,
    out_ref,
    send_buf,
    arrived,
    rows,
    gate_buf,
    up_buf,
    down_buf,
    hidden,
    part_send,
    part_recv,
    back_send,
    back,
    weigh,
    dispatch_send,
    dispatch_recv,
    forward_send,
    forward_recv,
    weight_send,
    weight_recv,
    weight_local,
    part_send_sem,
    part_recv_sem,
    back_send_sem,
    back_recv_sem,
    own_sem,
    mx_buf,
    mixer_weights,
    o_buf,
    q_buf,
    k_buf,
    v_buf,
    g_buf,
    inner_buf,
    update_buf,
    decay_buf,
    mix_buf,
    state_send,
    state_got,
    slab_send,
    slab_got,
    enter_send,
    enter_got,
    relay_got,
    side_got,
    load_sem,
    state_sems,
    relay_send,
    relay_recv,
    direct_send,
    direct_recv,
    summed_send,
    summed_recv,
):
    (nz, nx, nc), (z, x, c) = place()
    me = (z * nx + x) * nc + c
    y = lax.axis_index("tp")
    flip, mirror = y + 1 - 2 * (y % 2), 3 - y
    weight_peer = {"tp": (1 - c) * flip + c * mirror}
    token_peer = {"tp": (1 - c) * mirror + c * flip}
    experts = nz * nx * nc
    tokens, width = x_ref.shape
    piece = width // 4
    row_count = experts * CAP
    group = min(32, experts)
    group_count = experts // group

    slab = nx * nc
    spot = x * nc + c
    loads = [pltpu.make_async_copy(mx_hbm, mx_buf, load_sem.at[0])]
    for n, source in enumerate((q_hbm, k_hbm, v_hbm, g_hbm)):
        loads.append(pltpu.make_async_copy(source, mixer_weights.at[n], load_sem.at[1 + n]))
    loads.append(pltpu.make_async_copy(o_hbm, o_buf, load_sem.at[5]))

    barrier = pltpu.get_barrier_semaphore()
    for_each_peer(
        lambda device, index: pl.semaphore_signal(
            barrier, inc=1, device_id=device, device_id_type=MESH_ID
        )
    )
    for peer in (weight_peer, token_peer):
        pl.semaphore_signal(barrier, inc=1, device_id=peer, device_id_type=MESH_ID)
    locals_ = []
    for k, (source, target) in enumerate(
        ((gate_hbm, gate_buf), (up_hbm, up_buf), (down_hbm, down_buf))
    ):
        locals_.append(pltpu.make_async_copy(source, target.at[0], weight_local.at[k]))
        locals_[-1].start()
    for load in loads:
        load.start()
    pl.semaphore_wait(barrier, experts + 1)

    weights_out = [
        remote(gate_hbm, gate_buf.at[1], weight_send.at[0], weight_recv.at[0], weight_peer),
        remote(up_hbm, up_buf.at[1], weight_send.at[1], weight_recv.at[1], weight_peer),
        remote(down_hbm, down_buf.at[1], weight_send.at[2], weight_recv.at[2], weight_peer),
    ]
    for copy in weights_out:
        copy.start()

    floats = x_ref[...].astype(jnp.float32)
    scale = lax.rsqrt(jnp.mean(floats * floats, axis=-1, keepdims=True) + EPS)
    normed = (floats * scale * gain_ref[...]).astype(jnp.bfloat16)

    entries = 2 * tokens
    routes = routes_ref[...]
    named = lax.broadcasted_iota(jnp.int32, (experts, entries), 0) == routes
    named_bf = jnp.where(named, 1.0, 0.0).astype(jnp.bfloat16)
    earlier = lax.broadcasted_iota(jnp.int32, (entries, entries), 0) < lax.broadcasted_iota(
        jnp.int32, (entries, entries), 1
    )
    prior = dot(named_bf, jnp.where(earlier, 1.0, 0.0).astype(jnp.bfloat16))
    slot = jnp.sum(jnp.where(named, prior, 0.0), axis=0, keepdims=True).astype(jnp.int32)
    target = routes * CAP + slot
    first, second = target[:, :tokens], target[:, tokens:]
    scores = score_ref[...]
    shares = scores / jnp.sum(scores, axis=0, keepdims=True)

    packed = (8 * experts, tokens)
    ids = [packed_ids(packed, 0, j) for j in (None, 0, 1, 2)]
    picks = [
        jnp.where((i == first) | (i == second), 1.0, 0.0).astype(jnp.bfloat16) for i in ids
    ]
    last = normed[:, 3 * piece :]
    for j in range(3):
        chosen = jnp.concatenate([picks[0], picks[1 + j]], axis=1)
        source = jnp.concatenate([normed[:, j * piece : (j + 1) * piece], last], axis=0)
        send_buf[j] = dot(chosen, source).astype(jnp.bfloat16).reshape(experts, 8, piece)
        for_each_peer(
            lambda device, index, j=j: remote(
                send_buf.at[j, index],
                arrived.at[0, j, me],
                dispatch_send.at[j],
                dispatch_recv.at[j],
                device,
            ).start()
        )
        pltpu.make_async_copy(send_buf.at[j, me], arrived.at[0, j, me], own_sem.at[j]).start()

    for load in loads:
        load.wait()
    project_rows(mx_buf, mx_gain, mixer_weights, cos_ref, sin_ref, q_buf, k_buf, v_buf, g_buf)
    scan_blocks(logs_ref, log_rows_ref, q_buf, k_buf, v_buf, inner_buf, update_buf, decay_buf)
    block_count, heads = update_buf.shape[:2]
    share = HEAD // slab
    for h in range(heads):
        state = update_buf[0, h]
        decayed = decay_buf[0, h]
        for b in range(1, block_count):
            state = jnp.exp(decay_buf[b, h][0:1]) * state + update_buf[b, h]
            decayed = decayed + decay_buf[b, h]
        for n in range(slab):
            state_send[n, h, :share] = state[n * share : (n + 1) * share]
            state_send[n, h, share:] = decayed

    def for_slab(body):
        def step(i, carry):
            n = lax.rem(spot + i, slab)
            body(n, {"ep_1": n // nc, "ep_2": n % nc})
            return carry

        lax.fori_loop(1, slab, step, 0)

    for_slab(
        lambda n, device: remote(
            state_send.at[n], state_got.at[spot], state_sems.at[0], state_sems.at[1], device
        ).start()
    )
    state_got[spot] = state_send[spot]

    for n, i in enumerate(ids):
        shared = jnp.where(i == first, shares[0:1], 0.0) + jnp.where(
            i == second, shares[1:2], 0.0
        )
        turned = shared.T
        high = turned.astype(jnp.bfloat16)
        weigh[n, 0] = high
        weigh[n, 1] = (turned - high.astype(jnp.float32)).astype(jnp.bfloat16)

    shape = (group * CAP, group * 8)
    spread = [
        jnp.where(
            packed_ids(shape, 1, j) == lax.broadcasted_iota(jnp.int32, shape, 0), 1.0, 0.0
        ).astype(jnp.bfloat16)
        for j in (None, 0, 1, 2)
    ]
    spread_last = jnp.concatenate(spread[1:], axis=1)

    def unpack(side, j):
        block = arrived[side, j].reshape(8 * experts, piece)
        for g in range(group_count):
            rows[side, g * group * CAP : (g + 1) * group * CAP, j * piece : (j + 1) * piece] = dot(
                spread[0], block[g * group * 8 : (g + 1) * group * 8]
            ).astype(jnp.bfloat16)

    def unpack_last(side):
        blocks = [arrived[side, j].reshape(8 * experts, piece) for j in range(3)]
        for g in range(group_count):
            stacked = jnp.concatenate(
                [block[g * group * 8 : (g + 1) * group * 8] for block in blocks], axis=0
            )
            rows[side, g * group * CAP : (g + 1) * group * CAP, 3 * piece :] = dot(
                spread_last, stacked
            ).astype(jnp.bfloat16)

    wait_bytes(state_send.at[pl.ds(0, slab - 1)], state_sems.at[1])
    running = [jnp.zeros((share, HEAD), jnp.float32)] * heads
    decayed = [jnp.zeros((1, HEAD), jnp.float32)] * heads
    prefixes, prefix_decays = [], []
    for n in range(slab):
        prefixes.append(list(running))
        prefix_decays.append(list(decayed))
        for h in range(heads):
            log_total = state_got[n, h, share : share + 1]
            running[h] = jnp.exp(log_total) * running[h] + state_got[n, h, :share]
            decayed[h] = decayed[h] + log_total
    for h in range(heads):
        slab_send[h, :share] = running[h]
        slab_send[h, share:] = jnp.broadcast_to(decayed[h], (8, HEAD))

    def z_step(i, carry):
        remote(
            slab_send,
            slab_got.at[z],
            state_sems.at[2],
            state_sems.at[3],
            {"ep_0": lax.rem(z + i, nz)},
        ).start()
        return carry

    lax.fori_loop(1, nz, z_step, 0)
    slab_got[z] = slab_send[...]

    forwards = []

    def forward(j):
        wait_bytes(send_buf.at[j, pl.ds(0, experts - 1)], dispatch_recv.at[j])
        pltpu.make_async_copy(send_buf.at[j, me], arrived.at[0, j, me], own_sem.at[j]).wait()
        forwards.append(
            remote(
                arrived.at[0, j],
                arrived.at[1, j],
                forward_send.at[j],
                forward_recv.at[j],
                token_peer,
            )
        )
        forwards[-1].start()
        unpack(0, j)

    forward(0)
    wait_bytes(slab_got.at[pl.ds(0, nz - 1)], state_sems.at[3])
    for h in range(heads):
        entry = jnp.zeros((share, HEAD), jnp.float32)
        for n in range(nz):
            entry = jnp.where(
                n < z,
                jnp.exp(slab_got[n, h, share : share + 1]) * entry + slab_got[n, h, :share],
                entry,
            )
        for n in range(slab):
            enter_send[n, h] = jnp.exp(prefix_decays[n][h]) * entry + prefixes[n][h]
    for_slab(
        lambda n, device: remote(
            enter_send.at[n], enter_got.at[spot], state_sems.at[4], state_sems.at[5], device
        ).start()
    )
    enter_got[spot] = enter_send[spot]
    wait_bytes(enter_send.at[pl.ds(0, slab - 1)], state_sems.at[5])
    entering = [
        jnp.concatenate([enter_got[n, h] for n in range(slab)], axis=0) for h in range(heads)
    ]
    forward(1)
    finish_blocks(
        entering, q_buf, g_buf, inner_buf, update_buf, decay_buf, head_gain, o_buf, mix_buf
    )
    forward(2)
    unpack_last(0)

    def expand(side, half):
        source = rows[side]
        gate_part = dot(source, gate_buf[half])
        up_part = dot(source, up_buf[half])
        hidden[side, half] = (gate_part / (1.0 + jnp.exp(-gate_part)) * up_part).astype(
            jnp.bfloat16
        )

    locals_[0].wait()
    locals_[1].wait()
    expand(0, 0)
    for j in range(3):
        forwards[j].wait_recv()
        unpack(1, j)
    unpack_last(1)
    expand(1, 0)
    weights_out[0].wait_recv()
    weights_out[1].wait_recv()
    expand(1, 1)

    def contract(side, k):
        columns = slice(k * piece, (k + 1) * piece)
        return dot(hidden[side, 0], down_buf[0, :, columns]) + dot(
            hidden[side, 1], down_buf[1, :, columns]
        )

    locals_[2].wait()
    weights_out[2].wait_recv()
    parts = {}
    for k in (3, 0, 1, 2):
        part_send[k] = contract(1, k).astype(jnp.bfloat16)
        parts[k] = remote(
            part_send.at[k], part_recv.at[k], part_send_sem.at[k], part_recv_sem.at[k], token_peer
        )
        parts[k].start()

    unit = mix_buf.shape[0] // 4
    half = width // 2
    right, left = lax.rem(y + 1, 4), lax.rem(y + 3, 4)

    def slot_of(owner):
        return pl.ds(pl.multiple_of(owner * unit, unit), unit)

    opposite = slot_of(lax.rem(y + 2, 4))
    sides = ((right, slice(0, half), slice(half, width)), (left, slice(half, width), slice(0, half)))
    directs = []
    for n, (peer, relayed, plain) in enumerate(sides):
        directs.append(
            remote(
                mix_buf.at[opposite, relayed],
                relay_got.at[n],
                relay_send.at[n],
                relay_recv.at[n],
                {"tp": peer},
            )
        )
        directs.append(
            remote(
                mix_buf.at[slot_of(peer), plain],
                side_got.at[n, :, plain],
                direct_send.at[n],
                direct_recv.at[n],
                {"tp": peer},
            )
        )
    for copy in directs:
        copy.start()
    expand(0, 1)

    def total(k):
        own = contract(0, k)
        parts[k].wait_recv()
        return (own + part_recv[k].astype(jnp.float32)).astype(jnp.bfloat16)

    gather = [
        jnp.where(
            packed_ids((group * 8, group * CAP), 0, j)
            == lax.broadcasted_iota(jnp.int32, (group * 8, group * CAP), 1),
            1.0,
            0.0,
        ).astype(jnp.bfloat16)
        for j in (None, 0, 1, 2)
    ]
    tail = total(3)
    for j in range(3):
        body = total(j)
        for g in range(group_count):
            span = slice(g * group * CAP, (g + 1) * group * CAP)
            back_send[j, g * group : (g + 1) * group] = (
                (dot(gather[0], body[span]) + dot(gather[1 + j], tail[span]))
                .astype(jnp.bfloat16)
                .reshape(group, 8, piece)
            )
        for_each_peer(
            lambda device, index, j=j: remote(
                back_send.at[j, index],
                back.at[j, me],
                back_send_sem.at[j],
                back_recv_sem.at[j],
                device,
            ).start()
        )
        pltpu.make_async_copy(back_send.at[j, me], back.at[j, me], own_sem.at[j]).start()

    summed = []
    for n, (peer, relayed, plain) in enumerate(sides):
        directs[2 * n].wait_recv()
        mix_buf[slot_of(peer), relayed] = (
            mix_buf[slot_of(peer), relayed].astype(jnp.float32) + relay_got[n].astype(jnp.float32)
        ).astype(jnp.bfloat16)
        summed.append(
            remote(
                mix_buf.at[slot_of(peer), relayed],
                side_got.at[n, :, relayed],
                summed_send.at[n],
                summed_recv.at[n],
                {"tp": peer},
            )
        )
        summed[-1].start()
    for n in range(2):
        directs[2 * n + 1].wait_recv()
        summed[n].wait_recv()
    mixed_ref[...] = (
        mix_buf[slot_of(y), :].astype(jnp.float32)
        + side_got[0].astype(jnp.float32)
        + side_got[1].astype(jnp.float32)
    ).astype(jnp.bfloat16)

    rest = jnp.zeros((tokens, piece), jnp.float32)
    for j in range(3):
        wait_bytes(back_send.at[j, pl.ds(0, experts - 1)], back_recv_sem.at[j])
        pltpu.make_async_copy(back_send.at[j, me], back.at[j, me], own_sem.at[j]).wait()
        block = back[j].reshape(8 * experts, piece)
        out_ref[:, j * piece : (j + 1) * piece] = (
            dot(weigh[0, 0], block) + dot(weigh[0, 1], block)
        ).astype(jnp.bfloat16)
        rest = rest + dot(weigh[1 + j, 0], block) + dot(weigh[1 + j, 1], block)
    out_ref[:, 3 * piece :] = rest.astype(jnp.bfloat16)

    for copy in weights_out + forwards + list(parts.values()) + directs + summed:
        copy.wait_send()
    for j in range(3):
        wait_bytes(send_buf.at[j, pl.ds(0, experts - 1)], dispatch_send.at[j])
        wait_bytes(back_send.at[j, pl.ds(0, experts - 1)], back_send_sem.at[j])


    wait_bytes(state_send.at[pl.ds(0, slab - 1)], state_sems.at[0])
    wait_bytes(slab_got.at[pl.ds(0, nz - 1)], state_sems.at[2])
    wait_bytes(enter_send.at[pl.ds(0, slab - 1)], state_sems.at[4])


def on_device(
    mixer_input,
    mixer_gain,
    query_weight,
    key_weight,
    value_weight,
    gate_weight,
    head_gain,
    output_weight,
    log_decay,
    expert_input,
    expert_gain,
    routes,
    route_weight,
    expert_gate,
    expert_up,
    expert_down,
):
    tokens, width = expert_input.shape
    experts = lax.axis_size(EP)
    slab, slabs = lax.axis_size("ep_1") * lax.axis_size("ep_2"), lax.axis_size("ep_0")
    shard = expert_gate.shape[2]
    piece = width // 4
    row_count = experts * CAP
    mix_rows, heads = log_decay.shape
    mix_width = heads * HEAD
    block_count = mix_rows // BLOCK
    share = HEAD // slab
    unit = mix_rows // 4
    bf16, f32 = jnp.bfloat16, jnp.float32

    half_dim = HEAD // 2
    position = lax.axis_index(EP) * mix_rows + jnp.arange(mix_rows, dtype=jnp.int32)
    frequency = 10000.0 ** (-jnp.arange(half_dim, dtype=f32) / half_dim)
    angles = position.astype(f32)[:, None] * frequency[None, :]
    cosine, sine = jnp.cos(angles), jnp.sin(angles)
    cosine = jnp.concatenate([cosine, cosine], axis=1)
    sine = jnp.concatenate([-sine, sine], axis=1)
    log_rows = log_decay.T.reshape(heads, block_count, BLOCK).transpose(1, 0, 2)

    vmem = pl.BlockSpec(memory_space=pltpu.VMEM)
    anywhere = pl.BlockSpec(memory_space=pl.ANY)
    dma = pltpu.SemaphoreType.DMA
    return pl.pallas_call(
        layer_kernel,
        out_shape=(
            jax.ShapeDtypeStruct((unit, width), bf16),
            jax.ShapeDtypeStruct((tokens, width), bf16),
        ),
        in_specs=[vmem] * 4
        + [anywhere] * 4
        + [vmem]
        + [anywhere] * 4
        + [vmem, anywhere]
        + [vmem] * 4,
        out_specs=(vmem, vmem),
        scratch_shapes=[
            pltpu.VMEM((3, experts, 8, piece), bf16),
            pltpu.VMEM((2, 3, experts, 8, piece), bf16),
            pltpu.VMEM((2, row_count, width), bf16),
            pltpu.VMEM((2, width, shard), bf16),
            pltpu.VMEM((2, width, shard), bf16),
            pltpu.VMEM((2, shard, width), bf16),
            pltpu.VMEM((2, 2, row_count, shard), bf16),
            pltpu.VMEM((4, row_count, piece), bf16),
            pltpu.VMEM((4, row_count, piece), bf16),
            pltpu.VMEM((3, experts, 8, piece), bf16),
            pltpu.VMEM((3, experts, 8, piece), bf16),
            pltpu.VMEM((4, 2, tokens, 8 * experts), bf16),
        ]
        + [dma((3,))] * 7
        + [dma((4,))] * 2
        + [dma((3,))] * 3
        + [
            pltpu.VMEM((mix_rows, width), bf16),
            pltpu.VMEM((4, width, mix_width), bf16),
            pltpu.VMEM((mix_width, width), bf16),
            pltpu.VMEM((mix_rows, mix_width), bf16),
            pltpu.VMEM((mix_rows, mix_width), bf16),
            pltpu.VMEM((mix_rows, mix_width), bf16),
            pltpu.VMEM((mix_rows, mix_width), bf16),
            pltpu.VMEM((mix_rows, mix_width), f32),
            pltpu.VMEM((block_count, heads, HEAD, HEAD), f32),
            pltpu.VMEM((block_count, heads, 8, HEAD), f32),
            pltpu.VMEM((mix_rows, width), bf16),
            pltpu.VMEM((slab, heads, share + 8, HEAD), f32),
            pltpu.VMEM((slab, heads, share + 8, HEAD), f32),
            pltpu.VMEM((heads, share + 8, HEAD), f32),
            pltpu.VMEM((slabs, heads, share + 8, HEAD), f32),
            pltpu.VMEM((slab, heads, share, HEAD), f32),
            pltpu.VMEM((slab, heads, share, HEAD), f32),
            pltpu.VMEM((2, unit, width // 2), bf16),
            pltpu.VMEM((2, unit, width), bf16),
            dma((6,)),
            dma((6,)),
        ]
        + [dma((2,))] * 6,
        compiler_params=pltpu.CompilerParams(
            collective_id=0, has_side_effects=True, vmem_limit_bytes=VMEM_LIMIT
        ),
        name="layer",
    )(
        expert_input,
        expert_gain.reshape(1, width),
        routes.T.reshape(1, -1),
        route_weight.T,
        expert_gate[0],
        expert_up[0],
        expert_down[0],
        mixer_input,
        mixer_gain.reshape(1, width),
        query_weight,
        key_weight,
        value_weight,
        gate_weight,
        head_gain.reshape(1, mix_width),
        output_weight,
        log_decay,
        log_rows,
        cosine,
        sine,
    )


def solution(mesh):
    finer = Mesh(mesh.devices.reshape(8, 4, 2, mesh.shape["tp"]), ("ep_0", "ep_1", "ep_2", "tp"))
    placed = (
        P(EP, None),
        P(),
        P(None, "tp"),
        P(None, "tp"),
        P(None, "tp"),
        P(None, "tp"),
        P("tp"),
        P("tp", None),
        P(EP, "tp"),
        P(EP_TP, None),
        P(),
        P(EP_TP, None),
        P(EP_TP, None),
        P(EP, None, "tp"),
        P(EP, None, "tp"),
        P(EP, "tp", None),
    )
    return jax.shard_map(
        on_device,
        mesh=finer,
        in_specs=placed,
        out_specs=(P(EP_TP, None), P(EP_TP, None)),
        check_vma=False,
    )
```

```python
import functools

import jax
import jax.numpy as jnp
from jax import lax
from jax.experimental import pallas as pl
from jax.experimental.pallas import tpu as pltpu
from jax.sharding import Mesh
from jax.sharding import PartitionSpec as P

BLOCK = 128
EP = ("ep_0", "ep_1", "ep_2")
EP_TP = ("ep_0", "ep_1", "ep_2", "tp")
EPS = 1e-06
CAP = 6
CHUNKS = (1, 1, 1, 1, 1, 1)
HEAD = 128
FINE = 64
MESH_ID = pl.DeviceIdType.MESH
VMEM_LIMIT = 66060288


def z_order(count):
    steps = []
    for k in range(1, count // 2 + 1):
        steps.append(k)
        if count - k != k:
            steps.append(count - k)
    return steps + [0]


def place():
    sizes = tuple(lax.axis_size(name) for name in EP)
    spots = tuple(lax.axis_index(name) for name in EP)
    return sizes, spots


def for_each_peer(body):
    (nz, nx, nc), (z, x, c) = place()

    def step(i, carry):
        tx = lax.rem(x + i // nc, nx)
        tc = lax.rem(c + i % nc, nc)
        for offset in z_order(nz):
            tz = lax.rem(z + offset, nz)
            call = functools.partial(
                body, {"ep_0": tz, "ep_1": tx, "ep_2": tc}, (tz * nx + tx) * nc + tc
            )
            if offset == 0:
                pl.when(i > 0)(call)
            else:
                call()
        return carry

    lax.fori_loop(0, nx * nc, step, 0)


def remote(src, dst, send_sem, recv_sem, device):
    return pltpu.make_async_remote_copy(
        src_ref=src,
        dst_ref=dst,
        send_sem=send_sem,
        recv_sem=recv_sem,
        device_id=device,
        device_id_type=MESH_ID,
    )


def wait_bytes(ref, sem):
    pltpu.make_async_copy(ref, ref, sem).wait()


def folded_rows(shape, dim, group, count):
    fold = 8 // count
    row = lax.broadcasted_iota(jnp.int32, shape, dim)
    return ((row % fold) * count + (row % 8) // fold) * group + row // 8


def flag(condition):
    return jnp.where(condition, 1.0, 0.0).astype(jnp.bfloat16)


def dot(a, b):
    return jnp.dot(a, b, preferred_element_type=jnp.float32)


def dot_t(a, b, dims):
    return lax.dot_general(a, b, (dims, ((), ())), preferred_element_type=jnp.float32)


def project_rows(mx_buf, mx_gain, mixer_weights, cos_ref, sin_ref, q_buf, k_buf, v_buf, g_buf):
    row_count, width = mx_buf.shape
    step_rows = min(256, row_count)
    heads = q_buf.shape[1] // HEAD

    def step(i, carry):
        span = pl.ds(pl.multiple_of(i * step_rows, step_rows), step_rows)
        floats = mx_buf[span, :].astype(jnp.float32)
        scale = lax.rsqrt(jnp.mean(floats * floats, axis=-1, keepdims=True) + EPS)
        normed = (floats * scale * mx_gain[...]).astype(jnp.bfloat16)
        cosines, sines = [], []
        for a in range(step_rows // FINE):
            base_cos = cos_ref[pl.ds(FINE + i * (step_rows // FINE) + a, 1), :]
            base_sin = sin_ref[pl.ds(FINE + i * (step_rows // FINE) + a, 1), :]
            fine_cos, fine_sin = cos_ref[:FINE, :], sin_ref[:FINE, :]
            cosines.append(base_cos * fine_cos - base_sin * fine_sin)
            sines.append(base_sin * fine_cos + base_cos * fine_sin)
        cosine, sine = jnp.concatenate(cosines, axis=0), jnp.concatenate(sines, axis=0)
        for n, target in enumerate((q_buf, k_buf, v_buf, g_buf)):
            raw = dot(normed, mixer_weights[n]).astype(jnp.bfloat16)
            if n >= 2:
                target[span, :] = raw
                continue
            for h in range(heads):
                part = raw[:, h * HEAD : (h + 1) * HEAD].astype(jnp.float32)
                swapped = jnp.concatenate([part[:, HEAD // 2 :], part[:, : HEAD // 2]], axis=1)
                turned = part * cosine + swapped * sine
                if n == 1:
                    turned = turned * HEAD ** (-0.5)
                target[span, h * HEAD : (h + 1) * HEAD] = turned.astype(jnp.bfloat16)
        return carry

    lax.fori_loop(0, row_count // step_rows, step, 0)


def scan_blocks(log_rows_ref, q_buf, k_buf, v_buf, inner_buf, update_buf, decay_buf):
    block_count = q_buf.shape[0] // BLOCK
    heads = q_buf.shape[1] // HEAD
    row_ids = lax.broadcasted_iota(jnp.int32, (BLOCK, BLOCK), 0)
    col_ids = lax.broadcasted_iota(jnp.int32, (BLOCK, BLOCK), 1)
    lower = col_ids <= row_ids

    def step(b, carry):
        span = pl.ds(pl.multiple_of(b * BLOCK, BLOCK), BLOCK)
        wide = log_rows_ref[b]
        for h in range(heads):
            lanes = slice(h * HEAD, (h + 1) * HEAD)
            cum_col = jnp.sum(jnp.where(lower, wide[h : h + 1, :], 0.0), axis=1, keepdims=True)
            cum_row = jnp.broadcast_to(cum_col, (BLOCK, BLOCK)).T
            total = jnp.sum(wide[h : h + 1, :], axis=1, keepdims=True)
            q, k, v = q_buf[span, lanes], k_buf[span, lanes], v_buf[span, lanes]
            scaled = (k.astype(jnp.float32) * jnp.exp(total - cum_col)).astype(jnp.bfloat16)
            update_buf[b, h] = dot_t(scaled, v, ((0,), (0,)))
            decay_buf[b, h] = jnp.broadcast_to(total, (8, HEAD))
            decays = jnp.where(lower, jnp.exp(jnp.where(lower, cum_col - cum_row, 0.0)), 0.0)
            scores = dot_t(q, k, ((1,), (1,)))
            inner_buf[span, lanes] = dot((scores * decays).astype(jnp.bfloat16), v)
            q_buf[span, lanes] = (q.astype(jnp.float32) * jnp.exp(cum_col)).astype(jnp.bfloat16)
        return carry

    lax.fori_loop(0, block_count, step, 0)


def finish_blocks(
    entering, q_buf, g_buf, inner_buf, update_buf, decay_buf, head_gain, out_weight, out_buf
):
    block_count = q_buf.shape[0] // BLOCK
    heads = q_buf.shape[1] // HEAD

    def step(b, states):
        span = pl.ds(pl.multiple_of(b * BLOCK, BLOCK), BLOCK)
        following, hidden = [], []
        for h in range(heads):
            lanes = slice(h * HEAD, (h + 1) * HEAD)
            state = states[h]
            retained = inner_buf[span, lanes] + dot(q_buf[span, lanes], state.astype(jnp.bfloat16))
            factor = jnp.exp(decay_buf[b, h][0:1])
            following.append(factor * state + update_buf[b, h])
            centred = retained - jnp.mean(retained, axis=-1, keepdims=True)
            spread = jnp.mean(centred * centred, axis=-1, keepdims=True)
            gate = g_buf[span, lanes].astype(jnp.float32)
            hidden.append(
                (
                    centred
                    * lax.rsqrt(spread + EPS)
                    * head_gain[:, lanes]
                    * (gate / (1.0 + jnp.exp(-gate)))
                ).astype(jnp.bfloat16)
            )
        out_buf[span, :] = dot(jnp.concatenate(hidden, axis=1), out_weight[...]).astype(jnp.bfloat16)
        return tuple(following)

    lax.fori_loop(0, block_count, step, tuple(entering))


def layer_kernel(
    x_ref,
    gain_ref,
    routes_ref,
    score_ref,
    gate_hbm,
    up_hbm,
    down_hbm,
    mx_hbm,
    mx_gain,
    q_hbm,
    k_hbm,
    v_hbm,
    g_hbm,
    head_gain,
    o_hbm,
    log_rows_ref,
    cos_ref,
    sin_ref,
    mixed_ref,
    out_ref,
    picked,
    send_buf,
    arrived,
    passed,
    rows,
    gate_buf,
    up_buf,
    down_buf,
    part_send,
    part_recv,
    back_send,
    back,
    weigh,
    result_rows,
    total_buf,
    dispatch_send,
    dispatch_recv,
    forward_send,
    forward_recv,
    weight_send,
    weight_recv,
    weight_local,
    part_send_sem,
    part_recv_sem,
    back_send_sem,
    back_recv_sem,
    own_sem,
    mx_buf,
    mixer_weights,
    o_buf,
    q_buf,
    k_buf,
    v_buf,
    g_buf,
    inner_buf,
    update_buf,
    decay_buf,
    mix_buf,
    state_send,
    state_got,
    slab_send,
    slab_got,
    enter_send,
    enter_got,
    relay_got,
    side_got,
    load_sem,
    state_sems,
    relay_send,
    relay_recv,
    direct_send,
    direct_recv,
    summed_send,
    summed_recv,
):
    (nz, nx, nc), (z, x, c) = place()
    me = (z * nx + x) * nc + c
    y = lax.axis_index("tp")
    flip, mirror = y + 1 - 2 * (y % 2), 3 - y
    weight_peer = {"tp": (1 - c) * flip + c * mirror}
    token_peer = {"tp": (1 - c) * mirror + c * flip}
    experts = nz * nx * nc
    tokens, width = x_ref.shape
    group = min(32, experts)
    group_count = experts // group

    slab = nx * nc
    spot = x * nc + c
    loads = [pltpu.make_async_copy(mx_hbm, mx_buf, load_sem.at[0])]
    for n, source in enumerate((q_hbm, k_hbm, v_hbm, g_hbm)):
        loads.append(pltpu.make_async_copy(source, mixer_weights.at[n], load_sem.at[1 + n]))
    loads.append(pltpu.make_async_copy(o_hbm, o_buf, load_sem.at[5]))

    locals_ = []
    for k, (source, target) in enumerate(
        ((gate_hbm, gate_buf), (up_hbm, up_buf), (down_hbm, down_buf))
    ):
        locals_.append(pltpu.make_async_copy(source, target.at[0], weight_local.at[k]))

    barrier = pltpu.get_barrier_semaphore()
    for_each_peer(
        lambda device, index: pl.semaphore_signal(
            barrier, inc=1, device_id=device, device_id_type=MESH_ID
        )
    )
    for peer in (weight_peer, token_peer):
        pl.semaphore_signal(barrier, inc=1, device_id=peer, device_id_type=MESH_ID)
    for load in loads + locals_:
        load.start()

    floats = x_ref[...].astype(jnp.float32)
    scale = lax.rsqrt(jnp.mean(floats * floats, axis=-1, keepdims=True) + EPS)
    normed = (floats * scale * gain_ref[...]).astype(jnp.bfloat16)

    entries = 2 * tokens
    routes = routes_ref[...]
    named = lax.broadcasted_iota(jnp.int32, (experts, entries), 0) == routes
    named_bf = jnp.where(named, 1.0, 0.0).astype(jnp.bfloat16)
    earlier = lax.broadcasted_iota(jnp.int32, (entries, entries), 0) < lax.broadcasted_iota(
        jnp.int32, (entries, entries), 1
    )
    prior = dot(named_bf, jnp.where(earlier, 1.0, 0.0).astype(jnp.bfloat16))
    slot = jnp.sum(jnp.where(named, prior, 0.0), axis=0, keepdims=True).astype(jnp.int32)
    target = routes * CAP + slot
    first, second = target[:, :tokens], target[:, tokens:]
    scores = score_ref[...]
    shares = scores / jnp.sum(scores, axis=0, keepdims=True)

    places = (experts, tokens)
    firsts = [0]
    for count in CHUNKS:
        firsts.append(firsts[-1] + count)

    def slot_ids(n):
        return lax.broadcasted_iota(jnp.int32, places, 0) * CAP + n

    chosen = jnp.concatenate(
        [flag((slot_ids(n) == first) | (slot_ids(n) == second)) for n in range(CAP)], axis=0
    )
    picked[...] = dot(chosen, normed).astype(jnp.bfloat16)

    block = 8 * group
    spreads, gathers = {}, {}
    for count in sorted(set(CHUNKS)):
        square = (block, block)
        spreads[count] = flag(
            folded_rows(square, 1, group, count) == lax.broadcasted_iota(jnp.int32, square, 0)
        )
        gathers[count] = flag(
            folded_rows(square, 0, group, count) == lax.broadcasted_iota(jnp.int32, square, 1)
        )

    def spans(p):
        count = CHUNKS[p]
        piece = width * count // 8
        for q in range(8 // count):
            for r in range(count):
                yield r, slice(q * piece, (q + 1) * piece)

    def fold(p, source, base, target):
        count = CHUNKS[p]
        for g in range(group_count):
            lined = jnp.concatenate(
                [
                    source[base + r * experts + g * group : base + r * experts + (g + 1) * group, columns]
                    for r, columns in spans(p)
                ],
                axis=0,
            )
            target[p][g * group : (g + 1) * group] = (
                dot(gathers[count], lined).astype(jnp.bfloat16).reshape(group, 8, -1)
            )

    def unfold(p, source, store):
        count = CHUNKS[p]
        whole = source[...].reshape(8 * experts, -1)
        for g in range(group_count):
            lined = dot(spreads[count], whole[g * block : (g + 1) * block]).astype(jnp.bfloat16)
            for n, (r, columns) in enumerate(spans(p)):
                low = r * experts + g * group
                store(slice(low, low + group), columns, lined[n * group : (n + 1) * group])

    def exchange(p, source, target, send_sem, recv_sem):
        for_each_peer(
            lambda device, index: remote(
                source[p].at[index], target[p].at[me], send_sem.at[p], recv_sem.at[p], device
            ).start()
        )
        pltpu.make_async_copy(source[p].at[me], target[p].at[me], own_sem.at[p]).start()

    def exchanged(p, source, target, recv_sem):
        wait_bytes(source[p].at[pl.ds(0, experts - 1)], recv_sem.at[p])
        pltpu.make_async_copy(source[p].at[me], target[p].at[me], own_sem.at[p]).wait()

    chunks = range(len(CHUNKS))
    for p in chunks:
        fold(p, picked, firsts[p] * experts, send_buf)

    pl.semaphore_wait(barrier, experts + 1)
    weights_out = [
        remote(gate_hbm, gate_buf.at[1], weight_send.at[0], weight_recv.at[0], weight_peer),
        remote(up_hbm, up_buf.at[1], weight_send.at[1], weight_recv.at[1], weight_peer),
        remote(down_hbm, down_buf.at[1], weight_send.at[2], weight_recv.at[2], weight_peer),
    ]
    for copy in weights_out:
        copy.start()
    for p in chunks:
        exchange(p, send_buf, arrived, dispatch_send, dispatch_recv)

    for load in loads:
        load.wait()
    project_rows(mx_buf, mx_gain, mixer_weights, cos_ref, sin_ref, q_buf, k_buf, v_buf, g_buf)
    scan_blocks(log_rows_ref, q_buf, k_buf, v_buf, inner_buf, update_buf, decay_buf)
    block_count, heads = update_buf.shape[:2]
    share = HEAD // slab
    for h in range(heads):
        state = update_buf[0, h]
        decayed = decay_buf[0, h]
        for b in range(1, block_count):
            state = jnp.exp(decay_buf[b, h][0:1]) * state + update_buf[b, h]
            decayed = decayed + decay_buf[b, h]
        for n in range(slab):
            state_send[n, h, :share] = state[n * share : (n + 1) * share]
            state_send[n, h, share:] = decayed

    def for_slab(body):
        def step(i, carry):
            n = lax.rem(spot + i, slab)
            body(n, {"ep_1": n // nc, "ep_2": n % nc})
            return carry

        lax.fori_loop(1, slab, step, 0)

    for_slab(
        lambda n, device: remote(
            state_send.at[n], state_got.at[spot], state_sems.at[0], state_sems.at[1], device
        ).start()
    )
    state_got[spot] = state_send[spot]

    for p in chunks:
        turned = jnp.concatenate(
            [
                jnp.where(slot_ids(n) == first, shares[0:1], 0.0)
                + jnp.where(slot_ids(n) == second, shares[1:2], 0.0)
                for n in range(firsts[p], firsts[p + 1])
            ],
            axis=0,
        ).T
        high = turned.astype(jnp.bfloat16)
        weigh[p][:tokens] = high
        weigh[p][tokens:] = (turned - high.astype(jnp.float32)).astype(jnp.bfloat16)

    def unpack(side, p, source):
        def store(low, columns, value):
            rows[p][side, low, columns] = value

        unfold(p, source[p], store)

    forwards, parts, hiddens = {}, {}, {}

    def forward(p):
        exchanged(p, send_buf, arrived, dispatch_recv)
        forwards[p] = remote(
            arrived[p], passed[p], forward_send.at[p], forward_recv.at[p], token_peer
        )
        forwards[p].start()
        unpack(0, p, arrived)

    def contract(hidden):
        return dot(hidden, down_buf[...].reshape(-1, width))

    def compute(p):
        forwards[p].wait_recv()
        unpack(1, p, passed)
        own_rows = CHUNKS[p] * experts
        source = rows[p][...].reshape(2 * own_rows, width)
        halves = []
        for half in range(2):
            gate_part = dot(source, gate_buf[half])
            up_part = dot(source, up_buf[half])
            halves.append(
                (gate_part / (1.0 + jnp.exp(-gate_part)) * up_part).astype(jnp.bfloat16)
            )
        hidden = jnp.concatenate(halves, axis=1)
        part_send[p][...] = contract(hidden[own_rows:]).astype(jnp.bfloat16)
        parts[p] = remote(
            part_send[p], part_recv[p], part_send_sem.at[p], part_recv_sem.at[p], token_peer
        )
        parts[p].start()
        hiddens[p] = hidden[:own_rows]

    def give_back(p):
        own = contract(hiddens[p])
        parts[p].wait_recv()
        result = (own + part_recv[p][...].astype(jnp.float32)).astype(jnp.bfloat16)
        fold(p, result, 0, back_send)
        exchange(p, back_send, back, back_send_sem, back_recv_sem)

    def combine(p):
        exchanged(p, back_send, back, back_recv_sem)

        def store(low, columns, value):
            result_rows[p][low, columns] = value

        unfold(p, back[p], store)
        sums = dot(weigh[p][...], result_rows[p][...])
        part = sums[:tokens] + sums[tokens:]
        if p > 0:
            part = part + total_buf[...]
        if p < len(CHUNKS) - 1:
            total_buf[...] = part
        else:
            out_ref[...] = part.astype(jnp.bfloat16)

    forward(0)
    wait_bytes(state_send.at[pl.ds(0, slab - 1)], state_sems.at[1])
    running = [jnp.zeros((share, HEAD), jnp.float32)] * heads
    decayed = [jnp.zeros((1, HEAD), jnp.float32)] * heads
    prefixes, prefix_decays = [], []
    for n in range(slab):
        prefixes.append(list(running))
        prefix_decays.append(list(decayed))
        for h in range(heads):
            log_total = state_got[n, h, share : share + 1]
            running[h] = jnp.exp(log_total) * running[h] + state_got[n, h, :share]
            decayed[h] = decayed[h] + log_total
    for h in range(heads):
        slab_send[h, :share] = running[h]
        slab_send[h, share:] = jnp.broadcast_to(decayed[h], (8, HEAD))

    def z_step(i, carry):
        remote(
            slab_send,
            slab_got.at[z],
            state_sems.at[2],
            state_sems.at[3],
            {"ep_0": lax.rem(z + i, nz)},
        ).start()
        return carry

    lax.fori_loop(1, nz, z_step, 0)
    slab_got[z] = slab_send[...]

    forward(1)
    for k in range(2):
        locals_[k].wait()
        weights_out[k].wait_recv()
    locals_[2].wait()
    weights_out[2].wait_recv()
    compute(0)
    forward(2)
    wait_bytes(slab_got.at[pl.ds(0, nz - 1)], state_sems.at[3])
    for h in range(heads):
        entry = jnp.zeros((share, HEAD), jnp.float32)
        for n in range(nz):
            entry = jnp.where(
                n < z,
                jnp.exp(slab_got[n, h, share : share + 1]) * entry + slab_got[n, h, :share],
                entry,
            )
        for n in range(slab):
            enter_send[n, h] = jnp.exp(prefix_decays[n][h]) * entry + prefixes[n][h]
    for_slab(
        lambda n, device: remote(
            enter_send.at[n], enter_got.at[spot], state_sems.at[4], state_sems.at[5], device
        ).start()
    )
    enter_got[spot] = enter_send[spot]
    compute(1)
    give_back(0)
    forward(3)
    compute(2)
    wait_bytes(enter_send.at[pl.ds(0, slab - 1)], state_sems.at[5])
    entering = [
        jnp.concatenate([enter_got[n, h] for n in range(slab)], axis=0) for h in range(heads)
    ]
    give_back(1)
    forward(4)
    finish_blocks(
        entering, q_buf, g_buf, inner_buf, update_buf, decay_buf, head_gain, o_buf, mix_buf
    )
    compute(3)
    give_back(2)
    forward(5)
    compute(4)
    give_back(3)
    compute(5)
    unit = mix_buf.shape[0] // 4
    half = width // 2
    right, left = lax.rem(y + 1, 4), lax.rem(y + 3, 4)

    def slot_of(owner):
        return pl.ds(pl.multiple_of(owner * unit, unit), unit)

    opposite = slot_of(lax.rem(y + 2, 4))
    sides = ((right, slice(0, half), slice(half, width)), (left, slice(half, width), slice(0, half)))
    directs = []
    for n, (peer, relayed, plain) in enumerate(sides):
        directs.append(
            remote(
                mix_buf.at[opposite, relayed],
                relay_got.at[n],
                relay_send.at[n],
                relay_recv.at[n],
                {"tp": peer},
            )
        )
        directs.append(
            remote(
                mix_buf.at[slot_of(peer), plain],
                side_got.at[n, :, plain],
                direct_send.at[n],
                direct_recv.at[n],
                {"tp": peer},
            )
        )
    for copy in directs:
        copy.start()
    give_back(4)
    give_back(5)
    summed = []
    for n, (peer, relayed, plain) in enumerate(sides):
        directs[2 * n].wait_recv()
        mix_buf[slot_of(peer), relayed] = (
            mix_buf[slot_of(peer), relayed].astype(jnp.float32) + relay_got[n].astype(jnp.float32)
        ).astype(jnp.bfloat16)
        summed.append(
            remote(
                mix_buf.at[slot_of(peer), relayed],
                side_got.at[n, :, relayed],
                summed_send.at[n],
                summed_recv.at[n],
                {"tp": peer},
            )
        )
        summed[-1].start()
    combine(0)
    combine(1)
    combine(2)
    combine(3)
    for n in range(2):
        directs[2 * n + 1].wait_recv()
        summed[n].wait_recv()
    mixed_ref[...] = (
        mix_buf[slot_of(y), :].astype(jnp.float32)
        + side_got[0].astype(jnp.float32)
        + side_got[1].astype(jnp.float32)
    ).astype(jnp.bfloat16)

    combine(4)
    combine(5)
    for copy in (
        weights_out + list(forwards.values()) + list(parts.values()) + directs + summed
    ):
        copy.wait_send()
    for p in chunks:
        wait_bytes(send_buf[p].at[pl.ds(0, experts - 1)], dispatch_send.at[p])
        wait_bytes(back_send[p].at[pl.ds(0, experts - 1)], back_send_sem.at[p])
    wait_bytes(state_send.at[pl.ds(0, slab - 1)], state_sems.at[0])
    wait_bytes(slab_got.at[pl.ds(0, nz - 1)], state_sems.at[2])
    wait_bytes(enter_send.at[pl.ds(0, slab - 1)], state_sems.at[4])


def on_device(
    mixer_input,
    mixer_gain,
    query_weight,
    key_weight,
    value_weight,
    gate_weight,
    head_gain,
    output_weight,
    log_decay,
    expert_input,
    expert_gain,
    routes,
    route_weight,
    expert_gate,
    expert_up,
    expert_down,
):
    tokens, width = expert_input.shape
    experts = lax.axis_size(EP)
    slab, slabs = lax.axis_size("ep_1") * lax.axis_size("ep_2"), lax.axis_size("ep_0")
    shard = expert_gate.shape[2]
    messages = [
        pltpu.VMEM((experts, 8, width * count // 8), jnp.bfloat16) for count in CHUNKS
    ]
    chunk_rows = [pltpu.VMEM((count * experts, width), jnp.bfloat16) for count in CHUNKS]
    mix_rows, heads = log_decay.shape
    mix_width = heads * HEAD
    block_count = mix_rows // BLOCK
    share = HEAD // slab
    unit = mix_rows // 4
    bf16, f32 = jnp.bfloat16, jnp.float32

    half_dim = HEAD // 2
    lane = jnp.arange(HEAD, dtype=jnp.int32)
    frequency = 10000.0 ** (-(lane % half_dim).astype(f32) / half_dim)
    row = jnp.arange(FINE + mix_rows // FINE, dtype=jnp.int32)
    coarse = lax.axis_index(EP) * mix_rows + (row - FINE) * FINE
    position = jnp.where(row < FINE, row, coarse)
    angles = position.astype(f32)[:, None] * frequency[None, :]
    cosine = jnp.cos(angles)
    sine = jnp.where(lane < half_dim, -1.0, 1.0) * jnp.sin(angles)
    log_rows = log_decay.T.reshape(heads, block_count, BLOCK).transpose(1, 0, 2)

    vmem = pl.BlockSpec(memory_space=pltpu.VMEM)
    anywhere = pl.BlockSpec(memory_space=pltpu.HBM)
    dma = pltpu.SemaphoreType.DMA
    chunk_sems = dma((len(CHUNKS),))
    return pl.pallas_call(
        layer_kernel,
        out_shape=(
            jax.ShapeDtypeStruct((unit, width), bf16),
            jax.ShapeDtypeStruct((tokens, width), bf16),
        ),
        in_specs=[vmem] * 4
        + [anywhere] * 4
        + [vmem]
        + [anywhere] * 4
        + [vmem, anywhere]
        + [vmem] * 3,
        out_specs=(vmem, vmem),
        scratch_shapes=[
            pltpu.VMEM((CAP * experts, width), bf16),
            messages,
            messages,
            messages,
            [pltpu.VMEM((2, count * experts, width), bf16) for count in CHUNKS],
            pltpu.VMEM((2, width, shard), bf16),
            pltpu.VMEM((2, width, shard), bf16),
            pltpu.VMEM((2, shard, width), bf16),
            chunk_rows,
            chunk_rows,
            messages,
            messages,
            [pltpu.VMEM((2 * tokens, count * experts), bf16) for count in CHUNKS],
            chunk_rows,
            pltpu.VMEM((tokens, width), f32),
        ]
        + [chunk_sems] * 4
        + [dma((3,))] * 3
        + [chunk_sems] * 5
        + [
            pltpu.VMEM((mix_rows, width), bf16),
            pltpu.VMEM((4, width, mix_width), bf16),
            pltpu.VMEM((mix_width, width), bf16),
            pltpu.VMEM((mix_rows, mix_width), bf16),
            pltpu.VMEM((mix_rows, mix_width), bf16),
            pltpu.VMEM((mix_rows, mix_width), bf16),
            pltpu.VMEM((mix_rows, mix_width), bf16),
            pltpu.VMEM((mix_rows, mix_width), f32),
            pltpu.VMEM((block_count, heads, HEAD, HEAD), f32),
            pltpu.VMEM((block_count, heads, 8, HEAD), f32),
            pltpu.VMEM((mix_rows, width), bf16),
            pltpu.VMEM((slab, heads, share + 8, HEAD), f32),
            pltpu.VMEM((slab, heads, share + 8, HEAD), f32),
            pltpu.VMEM((heads, share + 8, HEAD), f32),
            pltpu.VMEM((slabs, heads, share + 8, HEAD), f32),
            pltpu.VMEM((slab, heads, share, HEAD), f32),
            pltpu.VMEM((slab, heads, share, HEAD), f32),
            pltpu.VMEM((2, unit, width // 2), bf16),
            pltpu.VMEM((2, unit, width), bf16),
            dma((6,)),
            dma((6,)),
        ]
        + [dma((2,))] * 6,
        compiler_params=pltpu.CompilerParams(
            collective_id=0, has_side_effects=True, vmem_limit_bytes=VMEM_LIMIT
        ),
        name="layer",
    )(
        expert_input,
        expert_gain.reshape(1, width),
        routes.T.reshape(1, -1),
        route_weight.T,
        expert_gate[0],
        expert_up[0],
        expert_down[0],
        mixer_input,
        mixer_gain.reshape(1, width),
        query_weight,
        key_weight,
        value_weight,
        gate_weight,
        head_gain.reshape(1, mix_width),
        output_weight,
        log_rows,
        cosine,
        sine,
    )


def solution(mesh):
    finer = Mesh(mesh.devices.reshape(8, 4, 2, mesh.shape["tp"]), ("ep_0", "ep_1", "ep_2", "tp"))
    placed = (
        P(EP, None),
        P(),
        P(None, "tp"),
        P(None, "tp"),
        P(None, "tp"),
        P(None, "tp"),
        P("tp"),
        P("tp", None),
        P(EP, "tp"),
        P(EP_TP, None),
        P(),
        P(EP_TP, None),
        P(EP_TP, None),
        P(EP, None, "tp"),
        P(EP, None, "tp"),
        P(EP, "tp", None),
    )
    return jax.shard_map(
        on_device,
        mesh=finer,
        in_specs=placed,
        out_specs=(P(EP_TP, None), P(EP_TP, None)),
        check_vma=False,
    )
```

```python
import functools

import jax
import jax.numpy as jnp
import numpy as np
from jax import lax
from jax.experimental import pallas as pl
from jax.experimental.pallas import tpu as pltpu
from jax.sharding import Mesh
from jax.sharding import PartitionSpec as P

BLOCK = 128
EP = ("ep_0", "ep_1", "ep_2")
EP_TP = ("ep_0", "ep_1", "ep_2", "tp")
EPS = 1e-06
CAP = 6
CHUNKS = (1, 1, 1, 1, 1, 1)
HEAD = 128
FINE = 64
TURN = 6.283185307179586
TURN_HIGH = 6.28125
TURN_MIDDLE = 2029.0 / 2.0**20
TURN_LOW = TURN - TURN_HIGH - TURN_MIDDLE
SETTLE = 2
MESH_ID = pl.DeviceIdType.MESH
VMEM_LIMIT = 66060288


def z_order(count):
    steps = []
    for k in range(1, count // 2 + 1):
        steps.append(k)
        if count - k != k:
            steps.append(count - k)
    return steps + [0]


def place():
    sizes = tuple(lax.axis_size(name) for name in EP)
    spots = tuple(lax.axis_index(name) for name in EP)
    return sizes, spots


def for_each_peer(body):
    (nz, nx, nc), (z, x, c) = place()

    def step(i, carry):
        tx = lax.rem(x + i // nc, nx)
        tc = lax.rem(c + i % nc, nc)
        for offset in z_order(nz):
            tz = lax.rem(z + offset, nz)
            call = functools.partial(
                body, {"ep_0": tz, "ep_1": tx, "ep_2": tc}, (tz * nx + tx) * nc + tc
            )
            if offset == 0:
                pl.when(i > 0)(call)
            else:
                call()
        return carry

    lax.fori_loop(0, nx * nc, step, 0)


def remote(src, dst, send_sem, recv_sem, device):
    return pltpu.make_async_remote_copy(
        src_ref=src,
        dst_ref=dst,
        send_sem=send_sem,
        recv_sem=recv_sem,
        device_id=device,
        device_id_type=MESH_ID,
    )


def wait_bytes(ref, sem):
    pltpu.make_async_copy(ref, ref, sem).wait()


def folded_rows(shape, dim, group, count):
    fold = 8 // count
    row = lax.broadcasted_iota(jnp.int32, shape, dim)
    return ((row % fold) * count + (row % 8) // fold) * group + row // 8


def flag(condition):
    return jnp.where(condition, 1.0, 0.0).astype(jnp.bfloat16)


def dot(a, b):
    return jnp.dot(a, b, preferred_element_type=jnp.float32)


def dot_t(a, b, dims):
    return lax.dot_general(a, b, (dims, ((), ())), preferred_element_type=jnp.float32)


def project_rows(mx_buf, mx_gain, mixer_weights, cos_ref, sin_ref, q_buf, k_buf, v_buf, g_buf):
    row_count, width = mx_buf.shape
    step_rows = min(256, row_count)
    heads = q_buf.shape[1] // HEAD

    def step(i, carry):
        span = pl.ds(pl.multiple_of(i * step_rows, step_rows), step_rows)
        floats = mx_buf[span, :].astype(jnp.float32)
        scale = lax.rsqrt(jnp.mean(floats * floats, axis=-1, keepdims=True) + EPS)
        normed = (floats * scale * mx_gain[...]).astype(jnp.bfloat16)
        cosines, sines = [], []
        for a in range(step_rows // FINE):
            base_cos = cos_ref[pl.ds(FINE + i * (step_rows // FINE) + a, 1), :]
            base_sin = sin_ref[pl.ds(FINE + i * (step_rows // FINE) + a, 1), :]
            fine_cos, fine_sin = cos_ref[:FINE, :], sin_ref[:FINE, :]
            cosines.append(base_cos * fine_cos - base_sin * fine_sin)
            sines.append(base_sin * fine_cos + base_cos * fine_sin)
        cosine, sine = jnp.concatenate(cosines, axis=0), jnp.concatenate(sines, axis=0)
        for n, target in enumerate((q_buf, k_buf, v_buf, g_buf)):
            raw = dot(normed, mixer_weights[n]).astype(jnp.bfloat16)
            if n >= 2:
                target[span, :] = raw
                continue
            for h in range(heads):
                part = raw[:, h * HEAD : (h + 1) * HEAD].astype(jnp.float32)
                swapped = jnp.concatenate([part[:, HEAD // 2 :], part[:, : HEAD // 2]], axis=1)
                turned = part * cosine + swapped * sine
                if n == 1:
                    turned = turned * HEAD ** (-0.5)
                target[span, h * HEAD : (h + 1) * HEAD] = turned.astype(jnp.bfloat16)
        return carry

    lax.fori_loop(0, row_count // step_rows, step, 0)


def scan_blocks(log_rows_ref, q_buf, k_buf, v_buf, inner_buf, update_buf, decay_buf):
    block_count = q_buf.shape[0] // BLOCK
    heads = q_buf.shape[1] // HEAD
    row_ids = lax.broadcasted_iota(jnp.int32, (BLOCK, BLOCK), 0)
    col_ids = lax.broadcasted_iota(jnp.int32, (BLOCK, BLOCK), 1)
    lower = col_ids <= row_ids

    def step(b, carry):
        span = pl.ds(pl.multiple_of(b * BLOCK, BLOCK), BLOCK)
        wide = log_rows_ref[b]
        for h in range(heads):
            lanes = slice(h * HEAD, (h + 1) * HEAD)
            cum_col = jnp.sum(jnp.where(lower, wide[h : h + 1, :], 0.0), axis=1, keepdims=True)
            cum_row = jnp.broadcast_to(cum_col, (BLOCK, BLOCK)).T
            total = jnp.sum(wide[h : h + 1, :], axis=1, keepdims=True)
            q, k, v = q_buf[span, lanes], k_buf[span, lanes], v_buf[span, lanes]
            scaled = (k.astype(jnp.float32) * jnp.exp(total - cum_col)).astype(jnp.bfloat16)
            update_buf[b, h] = dot_t(scaled, v, ((0,), (0,)))
            decay_buf[b, h] = jnp.broadcast_to(total, (8, HEAD))
            decays = jnp.where(lower, jnp.exp(jnp.where(lower, cum_col - cum_row, 0.0)), 0.0)
            scores = dot_t(q, k, ((1,), (1,)))
            inner_buf[span, lanes] = dot((scores * decays).astype(jnp.bfloat16), v)
            q_buf[span, lanes] = (q.astype(jnp.float32) * jnp.exp(cum_col)).astype(jnp.bfloat16)
        return carry

    lax.fori_loop(0, block_count, step, 0)


def finish_blocks(
    entering, q_buf, g_buf, inner_buf, update_buf, decay_buf, head_gain, out_weight, out_buf
):
    block_count = q_buf.shape[0] // BLOCK
    heads = q_buf.shape[1] // HEAD

    def step(b, states):
        span = pl.ds(pl.multiple_of(b * BLOCK, BLOCK), BLOCK)
        following, hidden = [], []
        for h in range(heads):
            lanes = slice(h * HEAD, (h + 1) * HEAD)
            state = states[h]
            retained = inner_buf[span, lanes] + dot(q_buf[span, lanes], state.astype(jnp.bfloat16))
            factor = jnp.exp(decay_buf[b, h][0:1])
            following.append(factor * state + update_buf[b, h])
            centred = retained - jnp.mean(retained, axis=-1, keepdims=True)
            spread = jnp.mean(centred * centred, axis=-1, keepdims=True)
            gate = g_buf[span, lanes].astype(jnp.float32)
            hidden.append(
                (
                    centred
                    * lax.rsqrt(spread + EPS)
                    * head_gain[:, lanes]
                    * (gate / (1.0 + jnp.exp(-gate)))
                ).astype(jnp.bfloat16)
            )
        out_buf[span, :] = dot(jnp.concatenate(hidden, axis=1), out_weight[...]).astype(jnp.bfloat16)
        return tuple(following)

    lax.fori_loop(0, block_count, step, tuple(entering))


def layer_kernel(
    x_hbm,
    gain_hbm,
    routes_hbm,
    score_hbm,
    gate_hbm,
    up_hbm,
    down_hbm,
    mx_hbm,
    mx_gain_hbm,
    q_hbm,
    k_hbm,
    v_hbm,
    g_hbm,
    head_gain_hbm,
    o_hbm,
    log_rows_hbm,
    rate_hbm,
    mixed_ref,
    out_ref,
    x_ref,
    gain_ref,
    routes_ref,
    score_ref,
    mx_gain,
    head_gain,
    log_rows_ref,
    rate_ref,
    cos_ref,
    sin_ref,
    small_sem,
    picked,
    send_buf,
    arrived,
    passed,
    rows,
    gate_buf,
    up_buf,
    down_buf,
    part_send,
    part_recv,
    back_send,
    back,
    weigh,
    result_rows,
    total_buf,
    dispatch_send,
    dispatch_recv,
    forward_send,
    forward_recv,
    weight_send,
    weight_recv,
    weight_local,
    part_send_sem,
    part_recv_sem,
    back_send_sem,
    back_recv_sem,
    own_sem,
    mx_buf,
    mixer_weights,
    o_buf,
    q_buf,
    k_buf,
    v_buf,
    g_buf,
    inner_buf,
    update_buf,
    decay_buf,
    mix_buf,
    state_send,
    state_got,
    slab_send,
    slab_got,
    enter_send,
    enter_got,
    relay_got,
    side_got,
    load_sem,
    state_sems,
    relay_send,
    relay_recv,
    direct_send,
    direct_recv,
    summed_send,
    summed_recv,
):
    (nz, nx, nc), (z, x, c) = place()
    me = (z * nx + x) * nc + c
    y = lax.axis_index("tp")
    flip, mirror = y + 1 - 2 * (y % 2), 3 - y
    weight_peer = {"tp": (1 - c) * flip + c * mirror}
    token_peer = {"tp": (1 - c) * mirror + c * flip}
    experts = nz * nx * nc
    tokens, width = x_hbm.shape
    group = min(32, experts)
    group_count = experts // group

    smalls = []
    for n, (source, kept) in enumerate(
        (
            (x_hbm, x_ref),
            (gain_hbm, gain_ref),
            (routes_hbm, routes_ref),
            (score_hbm, score_ref),
            (mx_gain_hbm, mx_gain),
            (head_gain_hbm, head_gain),
            (log_rows_hbm, log_rows_ref),
            (rate_hbm, rate_ref),
        )
    ):
        smalls.append(pltpu.make_async_copy(source, kept, small_sem.at[n]))
    slab = nx * nc
    spot = x * nc + c
    loads = [pltpu.make_async_copy(mx_hbm, mx_buf, load_sem.at[0])]
    for n, source in enumerate((q_hbm, k_hbm, v_hbm, g_hbm)):
        loads.append(pltpu.make_async_copy(source, mixer_weights.at[n], load_sem.at[1 + n]))
    loads.append(pltpu.make_async_copy(o_hbm, o_buf, load_sem.at[5]))

    locals_ = []
    for k, (source, target) in enumerate(
        ((gate_hbm, gate_buf), (up_hbm, up_buf), (down_hbm, down_buf))
    ):
        locals_.append(pltpu.make_async_copy(source, target.at[0], weight_local.at[k]))

    for load in smalls:
        load.start()
    barrier = pltpu.get_barrier_semaphore()
    for_each_peer(
        lambda device, index: pl.semaphore_signal(
            barrier, inc=1, device_id=device, device_id_type=MESH_ID
        )
    )
    for peer in (weight_peer, token_peer):
        pl.semaphore_signal(barrier, inc=1, device_id=peer, device_id_type=MESH_ID)
    for load in loads + locals_:
        load.start()

    pl.semaphore_wait(barrier, experts + 1)
    weights_out = [
        remote(gate_hbm, gate_buf.at[1], weight_send.at[0], weight_recv.at[0], weight_peer),
        remote(up_hbm, up_buf.at[1], weight_send.at[1], weight_recv.at[1], weight_peer),
        remote(down_hbm, down_buf.at[1], weight_send.at[2], weight_recv.at[2], weight_peer),
    ]
    for copy in weights_out:
        copy.start()
    for load in smalls[:4]:
        load.wait()
    floats = x_ref[...].astype(jnp.float32)
    scale = lax.rsqrt(jnp.mean(floats * floats, axis=-1, keepdims=True) + EPS)
    normed = (floats * scale * gain_ref[...]).astype(jnp.bfloat16)

    entries = 2 * tokens
    routes = routes_ref[...]
    named = lax.broadcasted_iota(jnp.int32, (experts, entries), 0) == routes
    named_bf = jnp.where(named, 1.0, 0.0).astype(jnp.bfloat16)
    earlier = lax.broadcasted_iota(jnp.int32, (entries, entries), 0) < lax.broadcasted_iota(
        jnp.int32, (entries, entries), 1
    )
    prior = dot(named_bf, jnp.where(earlier, 1.0, 0.0).astype(jnp.bfloat16))
    slot = jnp.sum(jnp.where(named, prior, 0.0), axis=0, keepdims=True).astype(jnp.int32)
    target = routes * CAP + slot
    first, second = target[:, :tokens], target[:, tokens:]
    scores = score_ref[...]
    shares = scores / jnp.sum(scores, axis=0, keepdims=True)

    places = (experts, tokens)
    firsts = [0]
    for count in CHUNKS:
        firsts.append(firsts[-1] + count)

    def slot_ids(n):
        return lax.broadcasted_iota(jnp.int32, places, 0) * CAP + n

    chosen = jnp.concatenate(
        [flag((slot_ids(n) == first) | (slot_ids(n) == second)) for n in range(CAP)], axis=0
    )
    picked[...] = dot(chosen, normed).astype(jnp.bfloat16)

    block = 8 * group
    spreads, gathers = {}, {}
    for count in sorted(set(CHUNKS)):
        square = (block, block)
        spreads[count] = flag(
            folded_rows(square, 1, group, count) == lax.broadcasted_iota(jnp.int32, square, 0)
        )
        gathers[count] = flag(
            folded_rows(square, 0, group, count) == lax.broadcasted_iota(jnp.int32, square, 1)
        )

    def spans(p):
        count = CHUNKS[p]
        piece = width * count // 8
        for q in range(8 // count):
            for r in range(count):
                yield r, slice(q * piece, (q + 1) * piece)

    def fold(p, source, base, target):
        count = CHUNKS[p]
        for g in range(group_count):
            lined = jnp.concatenate(
                [
                    source[base + r * experts + g * group : base + r * experts + (g + 1) * group, columns]
                    for r, columns in spans(p)
                ],
                axis=0,
            )
            target[p][g * group : (g + 1) * group] = (
                dot(gathers[count], lined).astype(jnp.bfloat16).reshape(group, 8, -1)
            )

    def unfold(p, source, store):
        count = CHUNKS[p]
        whole = source[...].reshape(8 * experts, -1)
        for g in range(group_count):
            lined = dot(spreads[count], whole[g * block : (g + 1) * block]).astype(jnp.bfloat16)
            for n, (r, columns) in enumerate(spans(p)):
                low = r * experts + g * group
                store(slice(low, low + group), columns, lined[n * group : (n + 1) * group])

    def exchange(p, source, target, send_sem, recv_sem):
        for_each_peer(
            lambda device, index: remote(
                source[p].at[index], target[p].at[me], send_sem.at[p], recv_sem.at[p], device
            ).start()
        )
        pltpu.make_async_copy(source[p].at[me], target[p].at[me], own_sem.at[p]).start()

    def exchanged(p, source, target, recv_sem):
        wait_bytes(source[p].at[pl.ds(0, experts - 1)], recv_sem.at[p])
        pltpu.make_async_copy(source[p].at[me], target[p].at[me], own_sem.at[p]).wait()

    chunks = range(len(CHUNKS))
    for p in chunks:
        fold(p, picked, firsts[p] * experts, send_buf)

    for p in chunks:
        exchange(p, send_buf, arrived, dispatch_send, dispatch_recv)

    for load in smalls[4:] + loads:
        load.wait()
    table = cos_ref.shape
    line = lax.broadcasted_iota(jnp.int32, table, 0)
    position = jnp.where(line < FINE, line, me * mx_buf.shape[0] + (line - FINE) * FINE)
    angles = position.astype(jnp.float32) * rate_ref[...]
    turns = jnp.floor(angles * (1.0 / TURN) + 0.5)
    angles = ((angles - turns * TURN_HIGH) - turns * TURN_MIDDLE) - turns * TURN_LOW
    cos_ref[...] = jnp.cos(angles)
    sin_ref[...] = jnp.where(
        lax.broadcasted_iota(jnp.int32, table, 1) < HEAD // 2, -1.0, 1.0
    ) * jnp.sin(angles)
    project_rows(mx_buf, mx_gain, mixer_weights, cos_ref, sin_ref, q_buf, k_buf, v_buf, g_buf)
    scan_blocks(log_rows_ref, q_buf, k_buf, v_buf, inner_buf, update_buf, decay_buf)
    block_count, heads = update_buf.shape[:2]
    share = HEAD // slab
    for h in range(heads):
        state = update_buf[0, h]
        decayed = decay_buf[0, h]
        for b in range(1, block_count):
            state = jnp.exp(decay_buf[b, h][0:1]) * state + update_buf[b, h]
            decayed = decayed + decay_buf[b, h]
        for n in range(slab):
            state_send[n, h, :share] = state[n * share : (n + 1) * share]
            state_send[n, h, share:] = decayed

    def for_slab(body):
        def step(i, carry):
            n = lax.rem(spot + i, slab)
            body(n, {"ep_1": n // nc, "ep_2": n % nc})
            return carry

        lax.fori_loop(1, slab, step, 0)

    for_slab(
        lambda n, device: remote(
            state_send.at[n], state_got.at[spot], state_sems.at[0], state_sems.at[1], device
        ).start()
    )
    state_got[spot] = state_send[spot]

    for p in chunks:
        turned = jnp.concatenate(
            [
                jnp.where(slot_ids(n) == first, shares[0:1], 0.0)
                + jnp.where(slot_ids(n) == second, shares[1:2], 0.0)
                for n in range(firsts[p], firsts[p + 1])
            ],
            axis=0,
        ).T
        high = turned.astype(jnp.bfloat16)
        weigh[p][:tokens] = high
        weigh[p][tokens:] = (turned - high.astype(jnp.float32)).astype(jnp.bfloat16)

    def unpack(side, p, source):
        def store(low, columns, value):
            rows[p][side, low, columns] = value

        unfold(p, source[p], store)

    forwards, parts, hiddens = {}, {}, {}

    def forward(p):
        exchanged(p, send_buf, arrived, dispatch_recv)
        forwards[p] = remote(
            arrived[p], passed[p], forward_send.at[p], forward_recv.at[p], token_peer
        )
        forwards[p].start()
        unpack(0, p, arrived)

    def contract(hidden):
        return dot(hidden, down_buf[...].reshape(-1, width))

    def compute(p):
        forwards[p].wait_recv()
        unpack(1, p, passed)
        own_rows = CHUNKS[p] * experts
        source = rows[p][...].reshape(2 * own_rows, width)
        halves = []
        for half in range(2):
            gate_part = dot(source, gate_buf[half])
            up_part = dot(source, up_buf[half])
            halves.append(
                (gate_part / (1.0 + jnp.exp(-gate_part)) * up_part).astype(jnp.bfloat16)
            )
        hidden = jnp.concatenate(halves, axis=1)
        part_send[p][...] = contract(hidden[own_rows:]).astype(jnp.bfloat16)
        parts[p] = remote(
            part_send[p], part_recv[p], part_send_sem.at[p], part_recv_sem.at[p], token_peer
        )
        parts[p].start()
        hiddens[p] = hidden[:own_rows]

    def give_back(p):
        own = contract(hiddens[p])
        parts[p].wait_recv()
        result = (own + part_recv[p][...].astype(jnp.float32)).astype(jnp.bfloat16)
        fold(p, result, 0, back_send)
        exchange(p, back_send, back, back_send_sem, back_recv_sem)

    def combine(p):
        exchanged(p, back_send, back, back_recv_sem)

        def store(low, columns, value):
            result_rows[p][low, columns] = value

        unfold(p, back[p], store)
        sums = dot(weigh[p][...], result_rows[p][...])
        part = sums[:tokens] + sums[tokens:]
        if p > 0:
            part = part + total_buf[...]
        if p < len(CHUNKS) - 1:
            total_buf[...] = part
        else:
            out_ref[...] = part.astype(jnp.bfloat16)

    forward(0)
    wait_bytes(state_send.at[pl.ds(0, slab - 1)], state_sems.at[1])
    running = [jnp.zeros((share, HEAD), jnp.float32)] * heads
    decayed = [jnp.zeros((1, HEAD), jnp.float32)] * heads
    prefixes, prefix_decays = [], []
    for n in range(slab):
        prefixes.append(list(running))
        prefix_decays.append(list(decayed))
        for h in range(heads):
            log_total = state_got[n, h, share : share + 1]
            running[h] = jnp.exp(log_total) * running[h] + state_got[n, h, :share]
            decayed[h] = decayed[h] + log_total
    for h in range(heads):
        slab_send[h, :share] = running[h]
        slab_send[h, share:] = jnp.broadcast_to(decayed[h], (8, HEAD))

    def z_step(i, carry):
        remote(
            slab_send,
            slab_got.at[z],
            state_sems.at[2],
            state_sems.at[3],
            {"ep_0": lax.rem(z + i, nz)},
        ).start()
        return carry

    lax.fori_loop(1, nz, z_step, 0)
    slab_got[z] = slab_send[...]

    forward(1)
    for k in range(2):
        locals_[k].wait()
        weights_out[k].wait_recv()
    locals_[2].wait()
    weights_out[2].wait_recv()
    compute(0)
    forward(2)
    wait_bytes(slab_got.at[pl.ds(0, nz - 1)], state_sems.at[3])
    for h in range(heads):
        entry = jnp.zeros((share, HEAD), jnp.float32)
        for n in range(nz):
            entry = jnp.where(
                n < z,
                jnp.exp(slab_got[n, h, share : share + 1]) * entry + slab_got[n, h, :share],
                entry,
            )
        for n in range(slab):
            enter_send[n, h] = jnp.exp(prefix_decays[n][h]) * entry + prefixes[n][h]
    for_slab(
        lambda n, device: remote(
            enter_send.at[n], enter_got.at[spot], state_sems.at[4], state_sems.at[5], device
        ).start()
    )
    enter_got[spot] = enter_send[spot]
    compute(1)
    give_back(0)
    forward(3)
    compute(2)
    wait_bytes(enter_send.at[pl.ds(0, slab - 1)], state_sems.at[5])
    entering = [
        jnp.concatenate([enter_got[n, h] for n in range(slab)], axis=0) for h in range(heads)
    ]
    give_back(1)
    forward(4)
    finish_blocks(
        entering, q_buf, g_buf, inner_buf, update_buf, decay_buf, head_gain, o_buf, mix_buf
    )
    compute(3)
    give_back(2)
    forward(5)
    compute(4)
    give_back(3)
    compute(5)
    unit = mix_buf.shape[0] // 4
    half = width // 2
    right, left = lax.rem(y + 1, 4), lax.rem(y + 3, 4)

    def slot_of(owner):
        return pl.ds(pl.multiple_of(owner * unit, unit), unit)

    opposite = slot_of(lax.rem(y + 2, 4))
    sides = ((right, slice(0, half), slice(half, width)), (left, slice(half, width), slice(0, half)))
    directs = []
    for n, (peer, relayed, plain) in enumerate(sides):
        directs.append(
            remote(
                mix_buf.at[opposite, relayed],
                relay_got.at[n],
                relay_send.at[n],
                relay_recv.at[n],
                {"tp": peer},
            )
        )
        directs.append(
            remote(
                mix_buf.at[slot_of(peer), plain],
                side_got.at[n, :, plain],
                direct_send.at[n],
                direct_recv.at[n],
                {"tp": peer},
            )
        )
    for copy in directs:
        copy.start()
    give_back(4)
    give_back(5)
    summed = []
    for n, (peer, relayed, plain) in enumerate(sides):
        directs[2 * n].wait_recv()
        mix_buf[slot_of(peer), relayed] = (
            mix_buf[slot_of(peer), relayed].astype(jnp.float32) + relay_got[n].astype(jnp.float32)
        ).astype(jnp.bfloat16)
        summed.append(
            remote(
                mix_buf.at[slot_of(peer), relayed],
                side_got.at[n, :, relayed],
                summed_send.at[n],
                summed_recv.at[n],
                {"tp": peer},
            )
        )
        summed[-1].start()
    combine(0)
    combine(1)
    combine(2)
    combine(3)
    for n in range(2):
        directs[2 * n + 1].wait_recv()
        summed[n].wait_recv()
    mixed_ref[...] = (
        mix_buf[slot_of(y), :].astype(jnp.float32)
        + side_got[0].astype(jnp.float32)
        + side_got[1].astype(jnp.float32)
    ).astype(jnp.bfloat16)

    combine(4)
    combine(5)
    for copy in (
        weights_out + list(forwards.values()) + list(parts.values()) + directs + summed
    ):
        copy.wait_send()
    for p in chunks:
        wait_bytes(send_buf[p].at[pl.ds(0, experts - 1)], dispatch_send.at[p])
        wait_bytes(back_send[p].at[pl.ds(0, experts - 1)], back_send_sem.at[p])
    wait_bytes(state_send.at[pl.ds(0, slab - 1)], state_sems.at[0])
    wait_bytes(slab_got.at[pl.ds(0, nz - 1)], state_sems.at[2])
    wait_bytes(enter_send.at[pl.ds(0, slab - 1)], state_sems.at[4])


def settle_kernel(mixed, routed, mixed_out, routed_out, mixed_buf, routed_buf, load_sem, store_sem):
    loads, stores = [], []
    for n, (source, kept, target) in enumerate(
        ((mixed, mixed_buf, mixed_out), (routed, routed_buf, routed_out))
    ):
        step = source.shape[0] // SETTLE
        for k in range(SETTLE):
            part = pl.ds(k * step, step)
            loads.append(pltpu.make_async_copy(source.at[part], kept.at[part], load_sem.at[n, k]))
            stores.append(pltpu.make_async_copy(kept.at[part], target.at[part], store_sem.at[n, k]))
    for load in loads:
        load.start()
    for load, store in zip(loads, stores):
        load.wait()
        store.start()
    for store in stores:
        store.wait()


def on_device(
    mixer_input,
    mixer_gain,
    query_weight,
    key_weight,
    value_weight,
    gate_weight,
    head_gain,
    output_weight,
    log_decay,
    expert_input,
    expert_gain,
    routes,
    route_weight,
    expert_gate,
    expert_up,
    expert_down,
):
    tokens, width = expert_input.shape
    experts = lax.axis_size(EP)
    slab, slabs = lax.axis_size("ep_1") * lax.axis_size("ep_2"), lax.axis_size("ep_0")
    shard = expert_gate.shape[2]
    messages = [
        pltpu.VMEM((experts, 8, width * count // 8), jnp.bfloat16) for count in CHUNKS
    ]
    chunk_rows = [pltpu.VMEM((count * experts, width), jnp.bfloat16) for count in CHUNKS]
    mix_rows, heads = log_decay.shape
    mix_width = heads * HEAD
    block_count = mix_rows // BLOCK
    share = HEAD // slab
    unit = mix_rows // 4
    bf16, f32 = jnp.bfloat16, jnp.float32

    half_dim = HEAD // 2
    rates = 10000.0 ** (-(np.arange(HEAD) % half_dim) / half_dim)
    rates = jnp.asarray(rates.reshape(1, HEAD).astype(np.float32))
    log_rows = log_decay.T.reshape(heads, block_count, BLOCK).transpose(1, 0, 2)

    vmem = pl.BlockSpec(memory_space=pltpu.VMEM)
    anywhere = pl.BlockSpec(memory_space=pl.ANY)
    dma = pltpu.SemaphoreType.DMA
    chunk_sems = dma((len(CHUNKS),))
    mixed, routed = pl.pallas_call(
        layer_kernel,
        out_shape=(
            jax.ShapeDtypeStruct((unit, width), bf16),
            jax.ShapeDtypeStruct((tokens, width), bf16),
        ),
        in_specs=[anywhere] * 17,
        out_specs=(vmem, vmem),
        scratch_shapes=[
            pltpu.VMEM((tokens, width), bf16),
            pltpu.VMEM((1, width), f32),
            pltpu.VMEM((1, 2 * tokens), jnp.int32),
            pltpu.VMEM((2, tokens), f32),
            pltpu.VMEM((1, width), f32),
            pltpu.VMEM((1, mix_width), f32),
            pltpu.VMEM((block_count, heads, BLOCK), f32),
            pltpu.VMEM((1, HEAD), f32),
            pltpu.VMEM((FINE + mix_rows // FINE, HEAD), f32),
            pltpu.VMEM((FINE + mix_rows // FINE, HEAD), f32),
            dma((8,)),
            pltpu.VMEM((CAP * experts, width), bf16),
            messages,
            messages,
            messages,
            [pltpu.VMEM((2, count * experts, width), bf16) for count in CHUNKS],
            pltpu.VMEM((2, width, shard), bf16),
            pltpu.VMEM((2, width, shard), bf16),
            pltpu.VMEM((2, shard, width), bf16),
            chunk_rows,
            chunk_rows,
            messages,
            messages,
            [pltpu.VMEM((2 * tokens, count * experts), bf16) for count in CHUNKS],
            chunk_rows,
            pltpu.VMEM((tokens, width), f32),
        ]
        + [chunk_sems] * 4
        + [dma((3,))] * 3
        + [chunk_sems] * 5
        + [
            pltpu.VMEM((mix_rows, width), bf16),
            pltpu.VMEM((4, width, mix_width), bf16),
            pltpu.VMEM((mix_width, width), bf16),
            pltpu.VMEM((mix_rows, mix_width), bf16),
            pltpu.VMEM((mix_rows, mix_width), bf16),
            pltpu.VMEM((mix_rows, mix_width), bf16),
            pltpu.VMEM((mix_rows, mix_width), bf16),
            pltpu.VMEM((mix_rows, mix_width), f32),
            pltpu.VMEM((block_count, heads, HEAD, HEAD), f32),
            pltpu.VMEM((block_count, heads, 8, HEAD), f32),
            pltpu.VMEM((mix_rows, width), bf16),
            pltpu.VMEM((slab, heads, share + 8, HEAD), f32),
            pltpu.VMEM((slab, heads, share + 8, HEAD), f32),
            pltpu.VMEM((heads, share + 8, HEAD), f32),
            pltpu.VMEM((slabs, heads, share + 8, HEAD), f32),
            pltpu.VMEM((slab, heads, share, HEAD), f32),
            pltpu.VMEM((slab, heads, share, HEAD), f32),
            pltpu.VMEM((2, unit, width // 2), bf16),
            pltpu.VMEM((2, unit, width), bf16),
            dma((6,)),
            dma((6,)),
        ]
        + [dma((2,))] * 6,
        compiler_params=pltpu.CompilerParams(
            collective_id=0, has_side_effects=True, vmem_limit_bytes=VMEM_LIMIT
        ),
        name="layer",
    )(
        expert_input,
        expert_gain.reshape(1, width),
        routes.T.reshape(1, -1),
        route_weight.T,
        expert_gate[0],
        expert_up[0],
        expert_down[0],
        mixer_input,
        mixer_gain.reshape(1, width),
        query_weight,
        key_weight,
        value_weight,
        gate_weight,
        head_gain.reshape(1, mix_width),
        output_weight,
        log_rows,
        rates,
    )
    return pl.pallas_call(
        settle_kernel,
        out_shape=(
            jax.ShapeDtypeStruct(mixed.shape, bf16),
            jax.ShapeDtypeStruct(routed.shape, bf16),
        ),
        in_specs=[anywhere] * 2,
        out_specs=(anywhere, anywhere),
        scratch_shapes=[
            pltpu.VMEM(mixed.shape, bf16),
            pltpu.VMEM(routed.shape, bf16),
            dma((2, SETTLE)),
            dma((2, SETTLE)),
        ],
        name="settle",
    )(mixed, routed)


def solution(mesh):
    finer = Mesh(mesh.devices.reshape(8, 4, 2, mesh.shape["tp"]), ("ep_0", "ep_1", "ep_2", "tp"))
    placed = (
        P(EP, None),
        P(),
        P(None, "tp"),
        P(None, "tp"),
        P(None, "tp"),
        P(None, "tp"),
        P("tp"),
        P("tp", None),
        P(EP, "tp"),
        P(EP_TP, None),
        P(),
        P(EP_TP, None),
        P(EP_TP, None),
        P(EP, None, "tp"),
        P(EP, None, "tp"),
        P(EP, "tp", None),
    )
    return jax.shard_map(
        on_device,
        mesh=finer,
        in_specs=placed,
        out_specs=(P(EP_TP, None), P(EP_TP, None)),
        check_vma=False,
    )
```

```python
import functools

import jax
import jax.numpy as jnp
import numpy as np
from jax import lax
from jax.experimental import pallas as pl
from jax.experimental.pallas import tpu as pltpu
from jax.sharding import Mesh
from jax.sharding import PartitionSpec as P

BLOCK = 128
EP = ("ep_0", "ep_1", "ep_2")
EP_TP = ("ep_0", "ep_1", "ep_2", "tp")
EPS = 1e-06
CAP = 6
CHUNKS = (1, 1, 1, 1, 1, 1)
HEAD = 128
FINE = 64
TURN = 6.283185307179586
TURN_HIGH = 6.28125
TURN_MIDDLE = 2029.0 / 2.0**20
TURN_LOW = TURN - TURN_HIGH - TURN_MIDDLE
SETTLE = 2
MESH_ID = pl.DeviceIdType.MESH
VMEM_LIMIT = 66060288


def z_order(count):
    steps = []
    for k in range(1, count // 2 + 1):
        steps.append(k)
        if count - k != k:
            steps.append(count - k)
    return steps + [0]


def place():
    sizes = tuple(lax.axis_size(name) for name in EP)
    spots = tuple(lax.axis_index(name) for name in EP)
    return sizes, spots


def for_each_peer(body):
    (nz, nx, nc), (z, x, c) = place()

    def step(i, carry):
        tx = lax.rem(x + i // nc, nx)
        tc = lax.rem(c + i % nc, nc)
        for offset in z_order(nz):
            tz = lax.rem(z + offset, nz)
            call = functools.partial(
                body, {"ep_0": tz, "ep_1": tx, "ep_2": tc}, (tz * nx + tx) * nc + tc
            )
            if offset == 0:
                pl.when(i > 0)(call)
            else:
                call()
        return carry

    lax.fori_loop(0, nx * nc, step, 0)


def remote(src, dst, send_sem, recv_sem, device):
    return pltpu.make_async_remote_copy(
        src_ref=src,
        dst_ref=dst,
        send_sem=send_sem,
        recv_sem=recv_sem,
        device_id=device,
        device_id_type=MESH_ID,
    )


def wait_bytes(ref, sem):
    pltpu.make_async_copy(ref, ref, sem).wait()


def folded_rows(shape, dim, group, count):
    fold = 8 // count
    row = lax.broadcasted_iota(jnp.int32, shape, dim)
    return ((row % fold) * count + (row % 8) // fold) * group + row // 8


def flag(condition):
    return jnp.where(condition, 1.0, 0.0).astype(jnp.bfloat16)


def dot(a, b):
    return jnp.dot(a, b, preferred_element_type=jnp.float32)


def dot_t(a, b, dims):
    return lax.dot_general(a, b, (dims, ((), ())), preferred_element_type=jnp.float32)


def project_rows(mx_buf, mx_gain, mixer_weights, cos_ref, sin_ref, q_buf, k_buf, v_buf, g_buf):
    row_count, width = mx_buf.shape
    step_rows = min(256, row_count)
    heads = q_buf.shape[1] // HEAD

    def step(i, carry):
        span = pl.ds(pl.multiple_of(i * step_rows, step_rows), step_rows)
        floats = mx_buf[span, :].astype(jnp.float32)
        scale = lax.rsqrt(jnp.mean(floats * floats, axis=-1, keepdims=True) + EPS)
        normed = (floats * scale * mx_gain[...]).astype(jnp.bfloat16)
        cosines, sines = [], []
        for a in range(step_rows // FINE):
            base_cos = cos_ref[pl.ds(FINE + i * (step_rows // FINE) + a, 1), :]
            base_sin = sin_ref[pl.ds(FINE + i * (step_rows // FINE) + a, 1), :]
            fine_cos, fine_sin = cos_ref[:FINE, :], sin_ref[:FINE, :]
            cosines.append(base_cos * fine_cos - base_sin * fine_sin)
            sines.append(base_sin * fine_cos + base_cos * fine_sin)
        cosine, sine = jnp.concatenate(cosines, axis=0), jnp.concatenate(sines, axis=0)
        for n, target in enumerate((q_buf, k_buf, v_buf, g_buf)):
            raw = dot(normed, mixer_weights[n]).astype(jnp.bfloat16)
            if n >= 2:
                target[span, :] = raw
                continue
            for h in range(heads):
                part = raw[:, h * HEAD : (h + 1) * HEAD].astype(jnp.float32)
                swapped = jnp.concatenate([part[:, HEAD // 2 :], part[:, : HEAD // 2]], axis=1)
                turned = part * cosine + swapped * sine
                if n == 1:
                    turned = turned * HEAD ** (-0.5)
                target[span, h * HEAD : (h + 1) * HEAD] = turned.astype(jnp.bfloat16)
        return carry

    lax.fori_loop(0, row_count // step_rows, step, 0)


def scan_blocks(log_rows_ref, q_buf, k_buf, v_buf, inner_buf, update_buf, decay_buf):
    block_count = q_buf.shape[0] // BLOCK
    heads = q_buf.shape[1] // HEAD
    row_ids = lax.broadcasted_iota(jnp.int32, (BLOCK, BLOCK), 0)
    col_ids = lax.broadcasted_iota(jnp.int32, (BLOCK, BLOCK), 1)
    lower = col_ids <= row_ids

    def step(b, carry):
        span = pl.ds(pl.multiple_of(b * BLOCK, BLOCK), BLOCK)
        wide = log_rows_ref[b]
        for h in range(heads):
            lanes = slice(h * HEAD, (h + 1) * HEAD)
            cum_col = jnp.sum(jnp.where(lower, wide[h : h + 1, :], 0.0), axis=1, keepdims=True)
            cum_row = jnp.broadcast_to(cum_col, (BLOCK, BLOCK)).T
            total = jnp.sum(wide[h : h + 1, :], axis=1, keepdims=True)
            q, k, v = q_buf[span, lanes], k_buf[span, lanes], v_buf[span, lanes]
            scaled = (k.astype(jnp.float32) * jnp.exp(total - cum_col)).astype(jnp.bfloat16)
            update_buf[b, h] = dot_t(scaled, v, ((0,), (0,)))
            decay_buf[b, h] = jnp.broadcast_to(total, (8, HEAD))
            decays = jnp.where(lower, jnp.exp(jnp.where(lower, cum_col - cum_row, 0.0)), 0.0)
            scores = dot_t(q, k, ((1,), (1,)))
            inner_buf[span, lanes] = dot((scores * decays).astype(jnp.bfloat16), v)
            q_buf[span, lanes] = (q.astype(jnp.float32) * jnp.exp(cum_col)).astype(jnp.bfloat16)
        return carry

    lax.fori_loop(0, block_count, step, 0)


def finish_blocks(
    entering, q_buf, g_buf, inner_buf, update_buf, decay_buf, head_gain, out_weight, out_buf
):
    block_count = q_buf.shape[0] // BLOCK
    heads = q_buf.shape[1] // HEAD

    def step(b, states):
        span = pl.ds(pl.multiple_of(b * BLOCK, BLOCK), BLOCK)
        following, hidden = [], []
        for h in range(heads):
            lanes = slice(h * HEAD, (h + 1) * HEAD)
            state = states[h]
            retained = inner_buf[span, lanes] + dot(q_buf[span, lanes], state.astype(jnp.bfloat16))
            factor = jnp.exp(decay_buf[b, h][0:1])
            following.append(factor * state + update_buf[b, h])
            centred = retained - jnp.mean(retained, axis=-1, keepdims=True)
            spread = jnp.mean(centred * centred, axis=-1, keepdims=True)
            gate = g_buf[span, lanes].astype(jnp.float32)
            hidden.append(
                (
                    centred
                    * lax.rsqrt(spread + EPS)
                    * head_gain[:, lanes]
                    * (gate / (1.0 + jnp.exp(-gate)))
                ).astype(jnp.bfloat16)
            )
        out_buf[span, :] = dot(jnp.concatenate(hidden, axis=1), out_weight[...]).astype(jnp.bfloat16)
        return tuple(following)

    lax.fori_loop(0, block_count, step, tuple(entering))


def layer_kernel(
    x_hbm,
    gain_hbm,
    routes_hbm,
    score_hbm,
    gate_hbm,
    up_hbm,
    down_hbm,
    mx_hbm,
    mx_gain_hbm,
    q_hbm,
    k_hbm,
    v_hbm,
    g_hbm,
    head_gain_hbm,
    o_hbm,
    log_rows_hbm,
    rate_hbm,
    mixed_ref,
    out_ref,
    x_ref,
    gain_ref,
    routes_ref,
    score_ref,
    mx_gain,
    head_gain,
    log_rows_ref,
    rate_ref,
    cos_ref,
    sin_ref,
    small_sem,
    picked,
    send_buf,
    arrived,
    passed,
    rows,
    gate_buf,
    up_buf,
    down_buf,
    part_send,
    part_recv,
    back_send,
    back,
    weigh,
    result_rows,
    total_buf,
    dispatch_send,
    dispatch_recv,
    forward_send,
    forward_recv,
    weight_send,
    weight_recv,
    weight_local,
    part_send_sem,
    part_recv_sem,
    back_send_sem,
    back_recv_sem,
    own_sem,
    mx_buf,
    mixer_weights,
    o_buf,
    q_buf,
    k_buf,
    v_buf,
    g_buf,
    inner_buf,
    update_buf,
    decay_buf,
    mix_buf,
    state_send,
    state_got,
    slab_send,
    slab_got,
    enter_send,
    enter_got,
    relay_got,
    side_got,
    load_sem,
    state_sems,
    relay_send,
    relay_recv,
    direct_send,
    direct_recv,
    summed_send,
    summed_recv,
):
    (nz, nx, nc), (z, x, c) = place()
    me = (z * nx + x) * nc + c
    y = lax.axis_index("tp")
    flip, mirror = y + 1 - 2 * (y % 2), 3 - y
    weight_peer = {"tp": (1 - c) * flip + c * mirror}
    token_peer = {"tp": (1 - c) * mirror + c * flip}
    experts = nz * nx * nc
    tokens, width = x_hbm.shape
    group = min(32, experts)
    group_count = experts // group

    smalls = []
    for n, (source, kept) in enumerate(
        (
            (x_hbm, x_ref),
            (gain_hbm, gain_ref),
            (routes_hbm, routes_ref),
            (score_hbm, score_ref),
            (mx_gain_hbm, mx_gain),
            (head_gain_hbm, head_gain),
            (log_rows_hbm, log_rows_ref),
            (rate_hbm, rate_ref),
        )
    ):
        smalls.append(pltpu.make_async_copy(source, kept, small_sem.at[n]))
    slab = nx * nc
    spot = x * nc + c
    loads = [pltpu.make_async_copy(mx_hbm, mx_buf, load_sem.at[0])]
    for n, source in enumerate((q_hbm, k_hbm, v_hbm, g_hbm)):
        loads.append(pltpu.make_async_copy(source, mixer_weights.at[n], load_sem.at[1 + n]))
    loads.append(pltpu.make_async_copy(o_hbm, o_buf, load_sem.at[5]))

    locals_ = []
    for k, (source, target) in enumerate(
        ((gate_hbm, gate_buf), (up_hbm, up_buf), (down_hbm, down_buf))
    ):
        locals_.append(pltpu.make_async_copy(source, target.at[0], weight_local.at[k]))

    for load in smalls:
        load.start()
    barrier = pltpu.get_barrier_semaphore()
    for_each_peer(
        lambda device, index: pl.semaphore_signal(
            barrier, inc=1, device_id=device, device_id_type=MESH_ID
        )
    )
    for peer in (weight_peer, token_peer):
        pl.semaphore_signal(barrier, inc=1, device_id=peer, device_id_type=MESH_ID)
    for load in loads + locals_:
        load.start()

    pl.semaphore_wait(barrier, experts + 1)
    weights_out = [
        remote(gate_hbm, gate_buf.at[1], weight_send.at[0], weight_recv.at[0], weight_peer),
        remote(up_hbm, up_buf.at[1], weight_send.at[1], weight_recv.at[1], weight_peer),
        remote(down_hbm, down_buf.at[1], weight_send.at[2], weight_recv.at[2], weight_peer),
    ]
    for copy in weights_out:
        copy.start()
    for load in smalls[:4]:
        load.wait()
    floats = x_ref[...].astype(jnp.float32)
    scale = lax.rsqrt(jnp.mean(floats * floats, axis=-1, keepdims=True) + EPS)
    normed = (floats * scale * gain_ref[...]).astype(jnp.bfloat16)

    entries = 2 * tokens
    routes = routes_ref[...]
    named = lax.broadcasted_iota(jnp.int32, (experts, entries), 0) == routes
    named_bf = jnp.where(named, 1.0, 0.0).astype(jnp.bfloat16)
    earlier = lax.broadcasted_iota(jnp.int32, (entries, entries), 0) < lax.broadcasted_iota(
        jnp.int32, (entries, entries), 1
    )
    prior = dot(named_bf, jnp.where(earlier, 1.0, 0.0).astype(jnp.bfloat16))
    slot = jnp.sum(jnp.where(named, prior, 0.0), axis=0, keepdims=True).astype(jnp.int32)
    target = routes * CAP + slot
    first, second = target[:, :tokens], target[:, tokens:]
    scores = score_ref[...]
    shares = scores / jnp.sum(scores, axis=0, keepdims=True)

    places = (experts, tokens)
    firsts = [0]
    for count in CHUNKS:
        firsts.append(firsts[-1] + count)

    def slot_ids(n):
        return lax.broadcasted_iota(jnp.int32, places, 0) * CAP + n

    chosen = jnp.concatenate(
        [flag((slot_ids(n) == first) | (slot_ids(n) == second)) for n in range(CAP)], axis=0
    )
    picked[...] = dot(chosen, normed).astype(jnp.bfloat16)

    block = 8 * group
    spreads, gathers = {}, {}
    for count in sorted(set(CHUNKS)):
        square = (block, block)
        spreads[count] = flag(
            folded_rows(square, 1, group, count) == lax.broadcasted_iota(jnp.int32, square, 0)
        )
        gathers[count] = flag(
            folded_rows(square, 0, group, count) == lax.broadcasted_iota(jnp.int32, square, 1)
        )

    def spans(p):
        count = CHUNKS[p]
        piece = width * count // 8
        for q in range(8 // count):
            for r in range(count):
                yield r, slice(q * piece, (q + 1) * piece)

    def fold(p, source, base, target):
        count = CHUNKS[p]
        for g in range(group_count):
            lined = jnp.concatenate(
                [
                    source[base + r * experts + g * group : base + r * experts + (g + 1) * group, columns]
                    for r, columns in spans(p)
                ],
                axis=0,
            )
            target[p][g * group : (g + 1) * group] = (
                dot(gathers[count], lined).astype(jnp.bfloat16).reshape(group, 8, -1)
            )

    def unfold(p, source, store):
        count = CHUNKS[p]
        whole = source[...].reshape(8 * experts, -1)
        for g in range(group_count):
            lined = dot(spreads[count], whole[g * block : (g + 1) * block]).astype(jnp.bfloat16)
            for n, (r, columns) in enumerate(spans(p)):
                low = r * experts + g * group
                store(slice(low, low + group), columns, lined[n * group : (n + 1) * group])

    def exchange(p, source, target, send_sem, recv_sem):
        for_each_peer(
            lambda device, index: remote(
                source[p].at[index], target[p].at[me], send_sem.at[p], recv_sem.at[p], device
            ).start()
        )
        pltpu.make_async_copy(source[p].at[me], target[p].at[me], own_sem.at[p]).start()

    def exchanged(p, source, target, recv_sem):
        wait_bytes(source[p].at[pl.ds(0, experts - 1)], recv_sem.at[p])
        pltpu.make_async_copy(source[p].at[me], target[p].at[me], own_sem.at[p]).wait()

    chunks = range(len(CHUNKS))
    for p in chunks:
        fold(p, picked, firsts[p] * experts, send_buf)

    for p in chunks:
        exchange(p, send_buf, arrived, dispatch_send, dispatch_recv)

    for load in smalls[4:] + loads:
        load.wait()
    table = cos_ref.shape
    line = lax.broadcasted_iota(jnp.int32, table, 0)
    position = jnp.where(line < FINE, line, me * mx_buf.shape[0] + (line - FINE) * FINE)
    angles = position.astype(jnp.float32) * rate_ref[...]
    turns = jnp.floor(angles * (1.0 / TURN) + 0.5)
    angles = ((angles - turns * TURN_HIGH) - turns * TURN_MIDDLE) - turns * TURN_LOW
    cos_ref[...] = jnp.cos(angles)
    sin_ref[...] = jnp.where(
        lax.broadcasted_iota(jnp.int32, table, 1) < HEAD // 2, -1.0, 1.0
    ) * jnp.sin(angles)
    project_rows(mx_buf, mx_gain, mixer_weights, cos_ref, sin_ref, q_buf, k_buf, v_buf, g_buf)
    scan_blocks(log_rows_ref, q_buf, k_buf, v_buf, inner_buf, update_buf, decay_buf)
    block_count, heads = update_buf.shape[:2]
    share = HEAD // slab
    for h in range(heads):
        state = update_buf[0, h]
        decayed = decay_buf[0, h]
        for b in range(1, block_count):
            state = jnp.exp(decay_buf[b, h][0:1]) * state + update_buf[b, h]
            decayed = decayed + decay_buf[b, h]
        for n in range(slab):
            state_send[n, h, :share] = state[n * share : (n + 1) * share]
            state_send[n, h, share:] = decayed

    def for_slab(body):
        def step(i, carry):
            n = lax.rem(spot + i, slab)
            body(n, {"ep_1": n // nc, "ep_2": n % nc})
            return carry

        lax.fori_loop(1, slab, step, 0)

    for_slab(
        lambda n, device: remote(
            state_send.at[n], state_got.at[spot], state_sems.at[0], state_sems.at[1], device
        ).start()
    )
    state_got[spot] = state_send[spot]

    for p in chunks:
        turned = jnp.concatenate(
            [
                jnp.where(slot_ids(n) == first, shares[0:1], 0.0)
                + jnp.where(slot_ids(n) == second, shares[1:2], 0.0)
                for n in range(firsts[p], firsts[p + 1])
            ],
            axis=0,
        ).T
        high = turned.astype(jnp.bfloat16)
        weigh[p][:tokens] = high
        weigh[p][tokens:] = (turned - high.astype(jnp.float32)).astype(jnp.bfloat16)

    def unpack(side, p, source):
        def store(low, columns, value):
            rows[p][side, low, columns] = value

        unfold(p, source[p], store)

    forwards, parts, hiddens = {}, {}, {}

    def forward(p):
        exchanged(p, send_buf, arrived, dispatch_recv)
        forwards[p] = remote(
            arrived[p], passed[p], forward_send.at[p], forward_recv.at[p], token_peer
        )
        forwards[p].start()
        unpack(0, p, arrived)

    def contract(hidden):
        return dot(hidden, down_buf[...].reshape(-1, width))

    def expand(p):
        forwards[p].wait_recv()
        unpack(1, p, passed)
        own_rows = CHUNKS[p] * experts
        source = rows[p][...].reshape(2 * own_rows, width)
        halves = []
        for half in range(2):
            gate_part = dot(source, gate_buf[half])
            up_part = dot(source, up_buf[half])
            halves.append(
                (gate_part / (1.0 + jnp.exp(-gate_part)) * up_part).astype(jnp.bfloat16)
            )
        hiddens[p] = jnp.concatenate(halves, axis=1)

    def project(p):
        own_rows = CHUNKS[p] * experts
        hidden = hiddens[p]
        part_send[p][...] = contract(hidden[own_rows:]).astype(jnp.bfloat16)
        parts[p] = remote(
            part_send[p], part_recv[p], part_send_sem.at[p], part_recv_sem.at[p], token_peer
        )
        parts[p].start()
        hiddens[p] = hidden[:own_rows]

    def give_back(p):
        own = contract(hiddens[p])
        parts[p].wait_recv()
        result = (own + part_recv[p][...].astype(jnp.float32)).astype(jnp.bfloat16)
        fold(p, result, 0, back_send)
        exchange(p, back_send, back, back_send_sem, back_recv_sem)

    def combine(p):
        exchanged(p, back_send, back, back_recv_sem)

        def store(low, columns, value):
            result_rows[p][low, columns] = value

        unfold(p, back[p], store)
        sums = dot(weigh[p][...], result_rows[p][...])
        part = sums[:tokens] + sums[tokens:]
        if p > 0:
            part = part + total_buf[...]
        if p < len(CHUNKS) - 1:
            total_buf[...] = part
        else:
            out_ref[...] = part.astype(jnp.bfloat16)

    forward(0)
    wait_bytes(state_send.at[pl.ds(0, slab - 1)], state_sems.at[1])
    running = [jnp.zeros((share, HEAD), jnp.float32)] * heads
    decayed = [jnp.zeros((1, HEAD), jnp.float32)] * heads
    prefixes, prefix_decays = [], []
    for n in range(slab):
        prefixes.append(list(running))
        prefix_decays.append(list(decayed))
        for h in range(heads):
            log_total = state_got[n, h, share : share + 1]
            running[h] = jnp.exp(log_total) * running[h] + state_got[n, h, :share]
            decayed[h] = decayed[h] + log_total
    for h in range(heads):
        slab_send[h, :share] = running[h]
        slab_send[h, share:] = jnp.broadcast_to(decayed[h], (8, HEAD))

    def z_step(i, carry):
        remote(
            slab_send,
            slab_got.at[z],
            state_sems.at[2],
            state_sems.at[3],
            {"ep_0": lax.rem(z + i, nz)},
        ).start()
        return carry

    lax.fori_loop(1, nz, z_step, 0)
    slab_got[z] = slab_send[...]

    forward(1)
    for k in range(2):
        locals_[k].wait()
        weights_out[k].wait_recv()
    expand(0)
    expand(1)
    locals_[2].wait()
    weights_out[2].wait_recv()
    project(0)
    forward(2)
    wait_bytes(slab_got.at[pl.ds(0, nz - 1)], state_sems.at[3])
    for h in range(heads):
        entry = jnp.zeros((share, HEAD), jnp.float32)
        for n in range(nz):
            entry = jnp.where(
                n < z,
                jnp.exp(slab_got[n, h, share : share + 1]) * entry + slab_got[n, h, :share],
                entry,
            )
        for n in range(slab):
            enter_send[n, h] = jnp.exp(prefix_decays[n][h]) * entry + prefixes[n][h]
    for_slab(
        lambda n, device: remote(
            enter_send.at[n], enter_got.at[spot], state_sems.at[4], state_sems.at[5], device
        ).start()
    )
    enter_got[spot] = enter_send[spot]
    project(1)
    give_back(0)
    forward(3)
    expand(2)
    project(2)
    wait_bytes(enter_send.at[pl.ds(0, slab - 1)], state_sems.at[5])
    entering = [
        jnp.concatenate([enter_got[n, h] for n in range(slab)], axis=0) for h in range(heads)
    ]
    give_back(1)
    forward(4)
    finish_blocks(
        entering, q_buf, g_buf, inner_buf, update_buf, decay_buf, head_gain, o_buf, mix_buf
    )
    expand(3)
    project(3)
    give_back(2)
    forward(5)
    expand(4)
    project(4)
    give_back(3)
    expand(5)
    project(5)
    unit = mix_buf.shape[0] // 4
    half = width // 2
    right, left = lax.rem(y + 1, 4), lax.rem(y + 3, 4)

    def slot_of(owner):
        return pl.ds(pl.multiple_of(owner * unit, unit), unit)

    opposite = slot_of(lax.rem(y + 2, 4))
    sides = ((right, slice(0, half), slice(half, width)), (left, slice(half, width), slice(0, half)))
    directs = []
    for n, (peer, relayed, plain) in enumerate(sides):
        directs.append(
            remote(
                mix_buf.at[opposite, relayed],
                relay_got.at[n],
                relay_send.at[n],
                relay_recv.at[n],
                {"tp": peer},
            )
        )
        directs.append(
            remote(
                mix_buf.at[slot_of(peer), plain],
                side_got.at[n, :, plain],
                direct_send.at[n],
                direct_recv.at[n],
                {"tp": peer},
            )
        )
    for copy in directs:
        copy.start()
    give_back(4)
    give_back(5)
    summed = []
    for n, (peer, relayed, plain) in enumerate(sides):
        directs[2 * n].wait_recv()
        mix_buf[slot_of(peer), relayed] = (
            mix_buf[slot_of(peer), relayed].astype(jnp.float32) + relay_got[n].astype(jnp.float32)
        ).astype(jnp.bfloat16)
        summed.append(
            remote(
                mix_buf.at[slot_of(peer), relayed],
                side_got.at[n, :, relayed],
                summed_send.at[n],
                summed_recv.at[n],
                {"tp": peer},
            )
        )
        summed[-1].start()
    combine(0)
    combine(1)
    combine(2)
    combine(3)
    combine(4)
    combine(5)
    for n in range(2):
        directs[2 * n + 1].wait_recv()
        summed[n].wait_recv()
    mixed_ref[...] = (
        mix_buf[slot_of(y), :].astype(jnp.float32)
        + side_got[0].astype(jnp.float32)
        + side_got[1].astype(jnp.float32)
    ).astype(jnp.bfloat16)

    for copy in (
        weights_out + list(forwards.values()) + list(parts.values()) + directs + summed
    ):
        copy.wait_send()
    for p in chunks:
        wait_bytes(send_buf[p].at[pl.ds(0, experts - 1)], dispatch_send.at[p])
        wait_bytes(back_send[p].at[pl.ds(0, experts - 1)], back_send_sem.at[p])
    wait_bytes(state_send.at[pl.ds(0, slab - 1)], state_sems.at[0])
    wait_bytes(slab_got.at[pl.ds(0, nz - 1)], state_sems.at[2])
    wait_bytes(enter_send.at[pl.ds(0, slab - 1)], state_sems.at[4])


def settle_kernel(mixed, routed, mixed_out, routed_out, mixed_buf, routed_buf, load_sem, store_sem):
    loads, stores = [], []
    for n, (source, kept, target) in enumerate(
        ((mixed, mixed_buf, mixed_out), (routed, routed_buf, routed_out))
    ):
        step = source.shape[0] // SETTLE
        for k in range(SETTLE):
            part = pl.ds(k * step, step)
            loads.append(pltpu.make_async_copy(source.at[part], kept.at[part], load_sem.at[n, k]))
            stores.append(pltpu.make_async_copy(kept.at[part], target.at[part], store_sem.at[n, k]))
    for load in loads:
        load.start()
    for load, store in zip(loads, stores):
        load.wait()
        store.start()
    for store in stores:
        store.wait()


def on_device(
    mixer_input,
    mixer_gain,
    query_weight,
    key_weight,
    value_weight,
    gate_weight,
    head_gain,
    output_weight,
    log_decay,
    expert_input,
    expert_gain,
    routes,
    route_weight,
    expert_gate,
    expert_up,
    expert_down,
):
    tokens, width = expert_input.shape
    experts = lax.axis_size(EP)
    slab, slabs = lax.axis_size("ep_1") * lax.axis_size("ep_2"), lax.axis_size("ep_0")
    shard = expert_gate.shape[2]
    messages = [
        pltpu.VMEM((experts, 8, width * count // 8), jnp.bfloat16) for count in CHUNKS
    ]
    chunk_rows = [pltpu.VMEM((count * experts, width), jnp.bfloat16) for count in CHUNKS]
    mix_rows, heads = log_decay.shape
    mix_width = heads * HEAD
    block_count = mix_rows // BLOCK
    share = HEAD // slab
    unit = mix_rows // 4
    bf16, f32 = jnp.bfloat16, jnp.float32

    half_dim = HEAD // 2
    rates = 10000.0 ** (-(np.arange(HEAD) % half_dim) / half_dim)
    rates = jnp.asarray(rates.reshape(1, HEAD).astype(np.float32))
    log_rows = log_decay.T.reshape(heads, block_count, BLOCK).transpose(1, 0, 2)

    vmem = pl.BlockSpec(memory_space=pltpu.VMEM)
    anywhere = pl.BlockSpec(memory_space=pl.ANY)
    dma = pltpu.SemaphoreType.DMA
    chunk_sems = dma((len(CHUNKS),))
    mixed, routed = pl.pallas_call(
        layer_kernel,
        out_shape=(
            jax.ShapeDtypeStruct((unit, width), bf16),
            jax.ShapeDtypeStruct((tokens, width), bf16),
        ),
        in_specs=[anywhere] * 17,
        out_specs=(vmem, vmem),
        scratch_shapes=[
            pltpu.VMEM((tokens, width), bf16),
            pltpu.VMEM((1, width), f32),
            pltpu.VMEM((1, 2 * tokens), jnp.int32),
            pltpu.VMEM((2, tokens), f32),
            pltpu.VMEM((1, width), f32),
            pltpu.VMEM((1, mix_width), f32),
            pltpu.VMEM((block_count, heads, BLOCK), f32),
            pltpu.VMEM((1, HEAD), f32),
            pltpu.VMEM((FINE + mix_rows // FINE, HEAD), f32),
            pltpu.VMEM((FINE + mix_rows // FINE, HEAD), f32),
            dma((8,)),
            pltpu.VMEM((CAP * experts, width), bf16),
            messages,
            messages,
            messages,
            [pltpu.VMEM((2, count * experts, width), bf16) for count in CHUNKS],
            pltpu.VMEM((2, width, shard), bf16),
            pltpu.VMEM((2, width, shard), bf16),
            pltpu.VMEM((2, shard, width), bf16),
            chunk_rows,
            chunk_rows,
            messages,
            messages,
            [pltpu.VMEM((2 * tokens, count * experts), bf16) for count in CHUNKS],
            chunk_rows,
            pltpu.VMEM((tokens, width), f32),
        ]
        + [chunk_sems] * 4
        + [dma((3,))] * 3
        + [chunk_sems] * 5
        + [
            pltpu.VMEM((mix_rows, width), bf16),
            pltpu.VMEM((4, width, mix_width), bf16),
            pltpu.VMEM((mix_width, width), bf16),
            pltpu.VMEM((mix_rows, mix_width), bf16),
            pltpu.VMEM((mix_rows, mix_width), bf16),
            pltpu.VMEM((mix_rows, mix_width), bf16),
            pltpu.VMEM((mix_rows, mix_width), bf16),
            pltpu.VMEM((mix_rows, mix_width), f32),
            pltpu.VMEM((block_count, heads, HEAD, HEAD), f32),
            pltpu.VMEM((block_count, heads, 8, HEAD), f32),
            pltpu.VMEM((mix_rows, width), bf16),
            pltpu.VMEM((slab, heads, share + 8, HEAD), f32),
            pltpu.VMEM((slab, heads, share + 8, HEAD), f32),
            pltpu.VMEM((heads, share + 8, HEAD), f32),
            pltpu.VMEM((slabs, heads, share + 8, HEAD), f32),
            pltpu.VMEM((slab, heads, share, HEAD), f32),
            pltpu.VMEM((slab, heads, share, HEAD), f32),
            pltpu.VMEM((2, unit, width // 2), bf16),
            pltpu.VMEM((2, unit, width), bf16),
            dma((6,)),
            dma((6,)),
        ]
        + [dma((2,))] * 6,
        compiler_params=pltpu.CompilerParams(
            collective_id=0, has_side_effects=True, vmem_limit_bytes=VMEM_LIMIT
        ),
        name="layer",
    )(
        expert_input,
        expert_gain.reshape(1, width),
        routes.T.reshape(1, -1),
        route_weight.T,
        expert_gate[0],
        expert_up[0],
        expert_down[0],
        mixer_input,
        mixer_gain.reshape(1, width),
        query_weight,
        key_weight,
        value_weight,
        gate_weight,
        head_gain.reshape(1, mix_width),
        output_weight,
        log_rows,
        rates,
    )
    return pl.pallas_call(
        settle_kernel,
        out_shape=(
            jax.ShapeDtypeStruct(mixed.shape, bf16),
            jax.ShapeDtypeStruct(routed.shape, bf16),
        ),
        in_specs=[anywhere] * 2,
        out_specs=(anywhere, anywhere),
        scratch_shapes=[
            pltpu.VMEM(mixed.shape, bf16),
            pltpu.VMEM(routed.shape, bf16),
            dma((2, SETTLE)),
            dma((2, SETTLE)),
        ],
        name="settle",
    )(mixed, routed)


def solution(mesh):
    finer = Mesh(mesh.devices.reshape(8, 4, 2, mesh.shape["tp"]), ("ep_0", "ep_1", "ep_2", "tp"))
    placed = (
        P(EP, None),
        P(),
        P(None, "tp"),
        P(None, "tp"),
        P(None, "tp"),
        P(None, "tp"),
        P("tp"),
        P("tp", None),
        P(EP, "tp"),
        P(EP_TP, None),
        P(),
        P(EP_TP, None),
        P(EP_TP, None),
        P(EP, None, "tp"),
        P(EP, None, "tp"),
        P(EP, "tp", None),
    )
    return jax.shard_map(
        on_device,
        mesh=finer,
        in_specs=placed,
        out_specs=(P(EP_TP, None), P(EP_TP, None)),
        check_vma=False,
    )
```
